32 devices in a mesh: fs: 8 (over z, x), tp: 4 (over y, core).
Axes of the slice: x: 2, y: 2, z: 4, core: 2. Of those that a mesh axis runs over, the one named last changes fastest.
Arguments:
- inputs: bfloat16 [1024, 2048], P('fs', 'tp'), may hold values from -6 to 6
- query_grad: bfloat16 [1024, 1024], P('fs', 'tp'), may hold values from -6 to 6
- forget_grad: bfloat16 [1024, 1024], P('fs', 'tp'), may hold values from -6 to 6
- forget_pre: bfloat16 [1024, 1024], P('fs', 'tp'), may hold values from -8 to 8
- lower_bound: float32 [1024], P('tp'), may hold values from 0.1 to 0.9
- query_weight: float32 [2048, 1024], P('fs', 'tp'), may hold values from -0.125 to 0.125
- forget_weight: float32 [2048, 1024], P('fs', 'tp'), may hold values from -0.125 to 0.125
- query_moment: float32 [2048, 1024], P('fs', 'tp'), may hold values from -6 to 6
- forget_moment: float32 [2048, 1024], P('fs', 'tp'), may hold values from -6 to 6
- query_rows: float32 [2048, 2048], P('fs'), may hold values from -0.6 to 0.6
- forget_rows: float32 [2048, 2048], P('fs'), may hold values from -0.6 to 0.6
- query_cols: float32 [8, 128, 128], P('tp'), may hold values from -0.6 to 0.6
- forget_cols: float32 [8, 128, 128], P('tp'), may hold values from -0.6 to 0.6
- query_row_root: bfloat16 [2048, 2048], P('fs'), may hold values from -2 to 2, as said below
- forget_row_root: bfloat16 [2048, 2048], P('fs'), may hold values from -2 to 2, as said below
- query_col_root: bfloat16 [8, 128, 128], P('tp'), may hold values from -2 to 2, as said below
- forget_col_root: bfloat16 [8, 128, 128], P('tp'), may hold values from -2 to 2, as said below
Outputs:
- query_master: float32 [2048, 1024], P('fs', 'tp')
- forget_master: float32 [2048, 1024], P('fs', 'tp')
- query_copy: bfloat16 [2048, 1024], P('fs', 'tp')
- forget_copy: bfloat16 [2048, 1024], P('fs', 'tp')
- query_step: float32 [2048, 1024], P('fs', 'tp')
- forget_step: float32 [2048, 1024], P('fs', 'tp')
- query_moment_next: float32 [2048, 1024], P('fs', 'tp')
- forget_moment_next: float32 [2048, 1024], P('fs', 'tp')
- query_rows_next: float32 [2048, 2048], P('fs')
- forget_rows_next: float32 [2048, 2048], P('fs')
- query_cols_next: float32 [8, 128, 128], P('tp')
- forget_cols_next: float32 [8, 128, 128], P('tp')
The draws below stay inside these ranges and needn't reach their ends.
Inputs may be any that keep to these rules, and one draw needn't show every extreme that they name: `query_row_root`: diagonal entries 0.5 to 1.5, the others of order 2048 ** -0.5. `forget_row_root`: diagonal entries 0.5 to 1.5, the others of order 2048 ** -0.5. `query_col_root`: diagonal entries 0.5 to 1.5, the others of order 128 ** -0.5. `forget_col_root`: diagonal entries 0.5 to 1.5, the others of order 128 ** -0.5.
All inputs are finite; a program needn't handle non-finite values.
Results may differ from the reference program's by a relative error of at most 0.005.
Values may be sent and summed in bfloat16 or wider, within the bound.
No kernel may reach another device: no remote copies, remote signals or barrier semaphores. Data moves between devices by JAX's collectives and lax.ppermute only.
A program may use at most 64 MiB of HBM per device.

```python
import jax
import jax.numpy as jnp
from jax import lax

D = 2048
HW = 1024
HEAD = 128
TOKENS = 1024
HEADS = 8


def root_matrix(key, shape):
    order = shape[-1]
    diag_key, spread_key = jax.random.split(key)
    spread = jnp.clip(jax.random.normal(spread_key, shape, jnp.float32), -4.0, 4.0) * order ** (-0.5)
    diagonal = jax.random.uniform(diag_key, shape[:-1], jnp.float32, 0.5, 1.5)
    unit_eye = jnp.eye(order, dtype=jnp.float32)
    return (spread * (1.0 - unit_eye) + diagonal[..., None] * unit_eye).astype(jnp.bfloat16)


def draw_query_row_root(key, part):
    return root_matrix(jax.random.fold_in(key, 11), (D, D))


def draw_forget_row_root(key, part):
    return root_matrix(jax.random.fold_in(key, 23), (D, D))


def draw_query_col_root(key, part):
    return root_matrix(jax.random.fold_in(key, 37), (HEADS, HEAD, HEAD))


def draw_forget_col_root(key, part):
    return root_matrix(jax.random.fold_in(key, 41), (HEADS, HEAD, HEAD))


def raised(entries, own_key, source, target, parts, factor):
    owner, partner = [(jnp.arange(entries.shape[dim]) // (entries.shape[dim] // parts)).reshape([-1 if axis == dim else 1 for axis in range(entries.ndim)]) for dim in (source, target)]
    chosen = jax.random.permutation(own_key, parts)[partner]
    strong = (owner == chosen) | (owner == (partner + parts // 2) % parts)
    return jnp.where(strong, factor * entries, entries)


def steps_of(rng, shape, shards, low, high):
    factor_of, own = 1.0, jax.random.fold_in(rng, 6)
    for dim, shards_of in shards:
        steps = jnp.exp(jax.random.uniform(jax.random.fold_in(own, dim), (shards_of,), jnp.float32, low / len(shards), high / len(shards)))
        factor_of = factor_of * jnp.repeat(steps, shape[dim] // shards_of).reshape([-1 if axis == dim else 1 for axis in range(len(shape))])
    return factor_of


def gaussian(rng, extent, deviation, bound, cuts=(), kind=jnp.bfloat16):
    array = jax.random.normal(rng, extent, jnp.float32) * deviation
    if len(cuts) > 0:
        array = steps_of(rng, extent, cuts, -0.22, 0.18) * array
    return jnp.clip(array, min=-bound, max=bound).astype(kind)


def bell_draw_with(key, extent, deviation, limit, shards, heavy, held_as=jnp.bfloat16):
    drawn = deviation * jax.random.normal(key, extent, jnp.float32)
    if shards:
        drawn = drawn * steps_of(key, extent, shards, -0.22, 0.18)
    return jnp.clip(raised(drawn, jax.random.fold_in(key, 3), *heavy), -limit, limit).astype(held_as)


def setup_inputs(seed: int = 0) -> dict:
    key_list = jax.random.split(jax.random.key(seed), 18)
    inputs = bell_draw_with(key_list[0], (TOKENS, D), 1.0, 6.0, ((0, 8), (1, 4)), (0, 1, 8, 2.0))
    query_grad = gaussian(key_list[1], (TOKENS, HW), 1.0, 6.0, ((0, 8), (1, 4)))
    forget_grad = gaussian(key_list[2], (TOKENS, HW), 1.0, 6.0, ((0, 8), (1, 4)))
    forget_pre = gaussian(key_list[3], (TOKENS, HW), 2.0, 8.0, ((0, 8), (1, 4)))
    lower_bound = jnp.clip(0.1 + 0.79999997 * jax.random.uniform(key_list[4], (HW,), jnp.float32) ** steps_of(key_list[4], (HW,), ((0, 4),), -0.2, 0.2), 0.1, 0.9)
    query_weight = gaussian(key_list[5], (D, HW), D ** -0.5, 0.125, ((0, 8), (1, 4)), jnp.float32)
    forget_weight = gaussian(key_list[6], (D, HW), D ** -0.5, 0.125, ((0, 8), (1, 4)), jnp.float32)
    query_moment = gaussian(key_list[7], (D, HW), 1.0, 6.0, ((0, 8), (1, 4)), jnp.float32)
    forget_moment = gaussian(key_list[8], (D, HW), 1.0, 6.0, ((0, 8), (1, 4)), jnp.float32)
    query_rows = gaussian(key_list[9], (D, D), 0.1, 0.6, ((0, 8),), jnp.float32)
    forget_rows = gaussian(key_list[10], (D, D), 0.1, 0.6, ((0, 8),), jnp.float32)
    query_cols = gaussian(key_list[11], (HEADS, HEAD, HEAD), 0.1, 0.6, ((0, 4),), jnp.float32)
    forget_cols = gaussian(key_list[12], (HEADS, HEAD, HEAD), 0.1, 0.6, ((0, 4),), jnp.float32)
    query_row_root = draw_query_row_root(jax.random.fold_in(key_list[17], 71), 0)
    forget_row_root = draw_forget_row_root(jax.random.fold_in(key_list[17], 71), 0)
    query_col_root = draw_query_col_root(jax.random.fold_in(key_list[17], 71), 0)
    forget_col_root = draw_forget_col_root(jax.random.fold_in(key_list[17], 71), 0)
    return dict(inputs=inputs, query_grad=query_grad, forget_grad=forget_grad, forget_pre=forget_pre, lower_bound=lower_bound, query_weight=query_weight, forget_weight=forget_weight, query_moment=query_moment, forget_moment=forget_moment, query_rows=query_rows, forget_rows=forget_rows, query_cols=query_cols, forget_cols=forget_cols, query_row_root=query_row_root, forget_row_root=forget_row_root, query_col_root=query_col_root, forget_col_root=forget_col_root)


stat_decay = 0.9
moment_decay = 0.9
learn_rate = 0.02
highest = lax.Precision.HIGHEST

def finish(gradient, weight, moment, rows, cols, row_root, col_root):
    square = jnp.sum(gradient * gradient)
    norm_scale = jnp.sqrt(D * HW / (square + 1.0))
    scaled = gradient * norm_scale
    rows_next = stat_decay * rows + (1.0 - stat_decay) / HW * jnp.dot(scaled, scaled.T, precision=highest)
    by_head = scaled.reshape(D, HEADS, HEAD)
    cols_next = stat_decay * cols + (1.0 - stat_decay) / D * jnp.einsum('rhi,rhj->hij', by_head, by_head, precision=highest)
    left_sum = jnp.dot(row_root.astype(jnp.float32), gradient, precision=highest)
    precond = norm_scale * jnp.einsum('rhi,hij->rhj', left_sum.reshape(D, HEADS, HEAD), col_root.astype(jnp.float32), precision=highest).reshape(D, HW)
    moment_next = moment_decay * moment + (1.0 - moment_decay) * precond
    update_step = moment_decay * moment_next + (1.0 - moment_decay) * precond
    master = weight - learn_rate * update_step
    return (master, master.astype(jnp.bfloat16), update_step, moment_next, rows_next, cols_next)

def reference(inputs, query_grad, forget_grad, forget_pre, lower_bound, query_weight, forget_weight, query_moment, forget_moment, query_rows, forget_rows, query_cols, forget_cols, query_row_root, forget_row_root, query_col_root, forget_col_root):
    sigma_gate = jax.nn.sigmoid(forget_pre.astype(jnp.float32))
    forget_cot = (forget_grad.astype(jnp.float32) * (1.0 - lower_bound) * sigma_gate * (1.0 - sigma_gate)).astype(jnp.bfloat16)
    query_gradient = jnp.dot(inputs.T, query_grad, preferred_element_type=jnp.float32)
    forget_gradient = jnp.dot(inputs.T, forget_cot, preferred_element_type=jnp.float32)
    query_out = finish(query_gradient, query_weight, query_moment, query_rows, query_cols, query_row_root, query_col_root)
    forget_out = finish(forget_gradient, forget_weight, forget_moment, forget_rows, forget_cols, forget_row_root, forget_col_root)
    return (query_out[0], forget_out[0], query_out[1], forget_out[1], query_out[2], forget_out[2], query_out[3], forget_out[3], query_out[4], forget_out[4], query_out[5], forget_out[5])
```

```python
from functools import partial

import jax
import jax.numpy as jnp
from jax import lax
from jax.sharding import PartitionSpec as P

D = 2048
HW = 1024
HEAD = 128


stat_decay = 0.9
moment_decay = 0.9
learn_rate = 0.02
highest = lax.Precision.HIGHEST


def fold_one(carry_state, shard_piece, offset, root_mine, grad_mine):
    left_sum, outer_rows, column_total = carry_state
    row_count, col_width = shard_piece.shape
    left_sum = left_sum + jnp.dot(root_mine, shard_piece, precision=highest)
    outer_piece = lax.dot_general(
        grad_mine, shard_piece, (((1,), (1,)), ((), ())), precision=highest
    )
    outer_rows = lax.dynamic_update_slice_in_dim(outer_rows, outer_piece, offset, 1)
    by_head = shard_piece.reshape(row_count, col_width // HEAD, HEAD)
    column_total = column_total + jnp.einsum("rhi,rhj->hij", by_head, by_head, precision=highest)
    return (left_sum, outer_rows, column_total)


def finish(weight, moment, rows, cols, col_root, left_sum, outer_rows, column_total, square):
    norm_scale = jnp.sqrt(D * HW / (square + 1.0))
    scale_twice = norm_scale * norm_scale
    rows_next = stat_decay * rows + (1.0 - stat_decay) / HW * scale_twice * outer_rows
    cols_next = stat_decay * cols + (1.0 - stat_decay) / D * scale_twice * column_total
    shard_rows, col_width = left_sum.shape
    shaped = left_sum.reshape(shard_rows, col_width // HEAD, HEAD)
    precond = norm_scale * jnp.einsum(
        "rhi,hij->rhj", shaped, col_root.astype(jnp.float32), precision=highest
    ).reshape(shard_rows, col_width)
    moment_next = moment_decay * moment + (1.0 - moment_decay) * precond
    update_step = moment_decay * moment_next + (1.0 - moment_decay) * precond
    master = weight - learn_rate * update_step
    return (master, master.astype(jnp.bfloat16), update_step, moment_next, rows_next, cols_next)


def summed_plan(
    inputs,
    query_grad,
    forget_cot,
    query_weight,
    forget_weight,
    query_moment,
    forget_moment,
    query_rows,
    forget_rows,
    query_cols,
    forget_cols,
    query_row_root,
    forget_row_root,
    query_col_root,
    forget_col_root,
):
    gathered = lax.all_gather(inputs, "tp", axis=1, tiled=True)
    shard_rows, col_width = query_weight.shape
    heads_here = col_width // HEAD
    row_roots = (query_row_root.astype(jnp.float32), forget_row_root.astype(jnp.float32))
    empty = (
        jnp.zeros((shard_rows, col_width), jnp.float32),
        jnp.zeros((shard_rows, D), jnp.float32),
        jnp.zeros((heads_here, HEAD, HEAD), jnp.float32),
    )
    joined = jnp.concatenate([query_grad, forget_cot], axis=1)
    summed = lax.psum_scatter(
        lax.dot_general(
            gathered, joined, (((0,), (0,)), ((), ())), preferred_element_type=jnp.float32
        ),
        "fs",
        scatter_dimension=0,
        tiled=True,
    )
    gradients = (summed[:, :col_width], summed[:, col_width:])
    offset = jnp.int32(0)
    results = (
        fold_one(
            empty,
            lax.all_gather(gradients[0].astype(jnp.bfloat16), "fs", axis=0, tiled=True).astype(
                jnp.float32
            ),
            offset,
            row_roots[0],
            gradients[0],
        ),
        fold_one(
            empty,
            lax.all_gather(gradients[1].astype(jnp.bfloat16), "fs", axis=0, tiled=True).astype(
                jnp.float32
            ),
            offset,
            row_roots[1],
            gradients[1],
        ),
    )
    query_trace = jnp.sum(jnp.diagonal(results[0][2], axis1=1, axis2=2))
    forget_trace = jnp.sum(jnp.diagonal(results[1][2], axis1=1, axis2=2))
    query_outer, forget_outer, query_square, forget_square = (
        lax.psum(results[0][1].astype(jnp.bfloat16), "tp").astype(jnp.float32),
        lax.psum(results[1][1].astype(jnp.bfloat16), "tp").astype(jnp.float32),
        lax.psum(query_trace.astype(jnp.bfloat16), "tp").astype(jnp.float32),
        lax.psum(forget_trace.astype(jnp.bfloat16), "tp").astype(jnp.float32),
    )
    query_out = finish(
        query_weight,
        query_moment,
        query_rows,
        query_cols,
        query_col_root,
        results[0][0],
        query_outer,
        results[0][2],
        query_square,
    )
    forget_out = finish(
        forget_weight,
        forget_moment,
        forget_rows,
        forget_cols,
        forget_col_root,
        results[1][0],
        forget_outer,
        results[1][2],
        forget_square,
    )
    return (
        query_out[0],
        forget_out[0],
        query_out[1],
        forget_out[1],
        query_out[2],
        forget_out[2],
        query_out[3],
        forget_out[3],
        query_out[4],
        forget_out[4],
        query_out[5],
        forget_out[5],
    )


def linear_pairs(fs_size, tp_size, target):
    pairs = []
    for f in range(fs_size):
        for t in range(tp_size):
            to_f, to_t = target(f, t)
            pairs.append((f * tp_size + t, to_f * tp_size + to_t))
    return pairs


def gather_operands(x_block, y_block, fs_size, tp_size):
    axes = ("fs", "tp")

    def move(value, target):
        return lax.ppermute(value, axes, linear_pairs(fs_size, tp_size, target))

    odd = lax.axis_index("tp") % 2 == 1

    def partner(f, t):
        return (f, t ^ 1)

    def first_hop(f, t):
        return (f ^ 1, t) if t % 2 == 0 else (f, t ^ 2)

    def second_hop(f, t):
        return (f, t ^ 2) if t % 2 == 0 else (f ^ 1, t)

    swapped = move(jnp.where(odd, x_block, y_block), partner)
    lane = jnp.stack([jnp.where(odd, swapped, x_block), jnp.where(odd, y_block, swapped)])
    lanes = [lane]
    for k in range(1, fs_size // 2):
        lanes.append(move(lane, lambda f, t, k=k: (f ^ (2 * k), t)))
    sets = []
    for lane in lanes:
        near = move(lane, first_hop)
        pair = jnp.stack([lane, near])
        far = move(pair, second_hop)
        quad = jnp.concatenate([pair, far])
        sets.append((quad, move(quad, partner)))
    return odd, sets


def gathered_plan(
    inputs,
    query_grad,
    forget_cot,
    query_weight,
    forget_weight,
    query_moment,
    forget_moment,
    query_rows,
    forget_rows,
    query_cols,
    forget_cols,
    query_row_root,
    forget_row_root,
    query_col_root,
    forget_col_root,
    fs_size,
    tp_size,
):
    rows_here, width = query_weight.shape
    odd, sets = gather_operands(
        inputs, jnp.concatenate([query_grad, forget_cot], axis=1), fs_size, tp_size
    )
    upper = lax.axis_index("tp") // 2 == 1
    mine_odd = lax.axis_index("tp") % 2
    x_all, y_all = [], []
    for own, other in sets:
        x_set = jnp.where(odd, other, own)
        y_set = jnp.where(odd, own, other)
        for p in range(2):
            halves = [jnp.concatenate([x_set[2 * h + p][0], x_set[2 * h + p][1]], axis=1) for h in range(2)]
            x_all.append(
                jnp.where(
                    upper,
                    jnp.concatenate([halves[1], halves[0]], axis=1),
                    jnp.concatenate([halves[0], halves[1]], axis=1),
                )
            )
            blocks = [y_set[2 * p + h][c] for h in range(2) for c in range(2)]
            y_all.append(
                jnp.concatenate([b[:, :width] for b in blocks] + [b[:, width:] for b in blocks], axis=1)
            )
    x_all = jnp.concatenate(x_all)
    y_all = jnp.concatenate(y_all)
    grad = lax.dot_general(
        x_all, y_all, (((0,), (0,)), ((), ())), preferred_element_type=jnp.float32
    ).astype(jnp.bfloat16)
    total = grad.shape[1] // 2
    first_row = lax.axis_index("fs") * rows_here
    out = []
    for i, (weight, moment, rows, cols, row_root, col_root) in enumerate(
        (
            (query_weight, query_moment, query_rows, query_cols, query_row_root, query_col_root),
            (forget_weight, forget_moment, forget_rows, forget_cols, forget_row_root, forget_col_root),
        )
    ):
        whole = grad[:, i * total : (i + 1) * total]
        square = jnp.sum(jnp.square(whole.astype(jnp.float32)))
        mine = lax.dynamic_slice_in_dim(whole, mine_odd * width, width, 1)
        band = lax.dynamic_slice_in_dim(whole, first_row, rows_here, 0)
        outer = lax.dot_general(
            band, whole, (((1,), (1,)), ((), ())), preferred_element_type=jnp.float32
        )
        by_head = mine.reshape(mine.shape[0], width // HEAD, HEAD)
        column_total = jnp.einsum(
            "rhi,rhj->hij", by_head, by_head, preferred_element_type=jnp.float32
        )
        left = jnp.dot(row_root, mine, preferred_element_type=jnp.float32)
        out.append(
            finish(weight, moment, rows, cols, col_root, left, outer, column_total, square)
        )
    return tuple(v for both in zip(*out) for v in both)


def use_gathered(tokens, model, hidden, fs_size, tp_size):
    blocks = fs_size // 2
    square_grid = tp_size == 4 and fs_size % 2 == 0 and blocks & (blocks - 1) == 0
    return square_grid and tokens * (model + 2 * hidden) <= model * 2 * hidden


def on_device(fs_size, tp_size, inputs, query_grad, forget_grad, forget_pre, lower_bound, *rest):
    sigma_gate = jax.nn.sigmoid(forget_pre.astype(jnp.float32))
    forget_cot = (
        forget_grad.astype(jnp.float32) * (1.0 - lower_bound) * sigma_gate * (1.0 - sigma_gate)
    ).astype(jnp.bfloat16)
    tokens = inputs.shape[0] * fs_size
    if use_gathered(tokens, inputs.shape[1] * tp_size, query_grad.shape[1] * tp_size, fs_size, tp_size):
        return gathered_plan(inputs, query_grad, forget_cot, *rest, fs_size, tp_size)
    return summed_plan(inputs, query_grad, forget_cot, *rest)


def solution(mesh):
    in_specs = (
        P("fs", "tp"),
        P("fs", "tp"),
        P("fs", "tp"),
        P("fs", "tp"),
        P("tp"),
        P("fs", "tp"),
        P("fs", "tp"),
        P("fs", "tp"),
        P("fs", "tp"),
        P("fs", None),
        P("fs", None),
        P("tp", None, None),
        P("tp", None, None),
        P("fs", None),
        P("fs", None),
        P("tp", None, None),
        P("tp", None, None),
    )
    out_specs = (
        P("fs", "tp"),
        P("fs", "tp"),
        P("fs", "tp"),
        P("fs", "tp"),
        P("fs", "tp"),
        P("fs", "tp"),
        P("fs", "tp"),
        P("fs", "tp"),
        P("fs", None),
        P("fs", None),
        P("tp", None, None),
        P("tp", None, None),
    )
    sizes = (mesh.shape["fs"], mesh.shape["tp"])
    return jax.shard_map(
        partial(on_device, *sizes), mesh=mesh, in_specs=in_specs, out_specs=out_specs, check_vma=False
    )
```

```python
from functools import partial

import jax
import jax.numpy as jnp
from jax import lax
from jax.experimental import pallas as pl
from jax.experimental.pallas import tpu as pltpu
from jax.sharding import PartitionSpec as P

D = 2048
HW = 1024
HEAD = 128


stat_decay = 0.9
moment_decay = 0.9
learn_rate = 0.02
highest = lax.Precision.HIGHEST


def fold_one(carry_state, shard_piece, offset, root_mine, grad_mine):
    left_sum, outer_rows, column_total = carry_state
    row_count, col_width = shard_piece.shape
    left_sum = left_sum + jnp.dot(root_mine, shard_piece, precision=highest)
    outer_piece = lax.dot_general(
        grad_mine, shard_piece, (((1,), (1,)), ((), ())), precision=highest
    )
    outer_rows = lax.dynamic_update_slice_in_dim(outer_rows, outer_piece, offset, 1)
    by_head = shard_piece.reshape(row_count, col_width // HEAD, HEAD)
    column_total = column_total + jnp.einsum("rhi,rhj->hij", by_head, by_head, precision=highest)
    return (left_sum, outer_rows, column_total)


def finish(weight, moment, rows, cols, col_root, left_sum, outer_rows, column_total, square):
    norm_scale = jnp.sqrt(D * HW / (square + 1.0))
    scale_twice = norm_scale * norm_scale
    rows_next = stat_decay * rows + (1.0 - stat_decay) / HW * scale_twice * outer_rows
    cols_next = stat_decay * cols + (1.0 - stat_decay) / D * scale_twice * column_total
    shard_rows, col_width = left_sum.shape
    shaped = left_sum.reshape(shard_rows, col_width // HEAD, HEAD)
    precond = norm_scale * jnp.einsum(
        "rhi,hij->rhj", shaped, col_root.astype(jnp.float32), precision=highest
    ).reshape(shard_rows, col_width)
    moment_next = moment_decay * moment + (1.0 - moment_decay) * precond
    update_step = moment_decay * moment_next + (1.0 - moment_decay) * precond
    master = weight - learn_rate * update_step
    return (master, master.astype(jnp.bfloat16), update_step, moment_next, rows_next, cols_next)


def summed_plan(
    inputs,
    query_grad,
    forget_cot,
    query_weight,
    forget_weight,
    query_moment,
    forget_moment,
    query_rows,
    forget_rows,
    query_cols,
    forget_cols,
    query_row_root,
    forget_row_root,
    query_col_root,
    forget_col_root,
):
    gathered = lax.all_gather(inputs, "tp", axis=1, tiled=True)
    shard_rows, col_width = query_weight.shape
    heads_here = col_width // HEAD
    row_roots = (query_row_root.astype(jnp.float32), forget_row_root.astype(jnp.float32))
    empty = (
        jnp.zeros((shard_rows, col_width), jnp.float32),
        jnp.zeros((shard_rows, D), jnp.float32),
        jnp.zeros((heads_here, HEAD, HEAD), jnp.float32),
    )
    joined = jnp.concatenate([query_grad, forget_cot], axis=1)
    summed = lax.psum_scatter(
        lax.dot_general(
            gathered, joined, (((0,), (0,)), ((), ())), preferred_element_type=jnp.float32
        ),
        "fs",
        scatter_dimension=0,
        tiled=True,
    )
    gradients = (summed[:, :col_width], summed[:, col_width:])
    offset = jnp.int32(0)
    results = (
        fold_one(
            empty,
            lax.all_gather(gradients[0].astype(jnp.bfloat16), "fs", axis=0, tiled=True).astype(
                jnp.float32
            ),
            offset,
            row_roots[0],
            gradients[0],
        ),
        fold_one(
            empty,
            lax.all_gather(gradients[1].astype(jnp.bfloat16), "fs", axis=0, tiled=True).astype(
                jnp.float32
            ),
            offset,
            row_roots[1],
            gradients[1],
        ),
    )
    query_trace = jnp.sum(jnp.diagonal(results[0][2], axis1=1, axis2=2))
    forget_trace = jnp.sum(jnp.diagonal(results[1][2], axis1=1, axis2=2))
    query_outer, forget_outer, query_square, forget_square = (
        lax.psum(results[0][1].astype(jnp.bfloat16), "tp").astype(jnp.float32),
        lax.psum(results[1][1].astype(jnp.bfloat16), "tp").astype(jnp.float32),
        lax.psum(query_trace.astype(jnp.bfloat16), "tp").astype(jnp.float32),
        lax.psum(forget_trace.astype(jnp.bfloat16), "tp").astype(jnp.float32),
    )
    query_out = finish(
        query_weight,
        query_moment,
        query_rows,
        query_cols,
        query_col_root,
        results[0][0],
        query_outer,
        results[0][2],
        query_square,
    )
    forget_out = finish(
        forget_weight,
        forget_moment,
        forget_rows,
        forget_cols,
        forget_col_root,
        results[1][0],
        forget_outer,
        results[1][2],
        forget_square,
    )
    return (
        query_out[0],
        forget_out[0],
        query_out[1],
        forget_out[1],
        query_out[2],
        forget_out[2],
        query_out[3],
        forget_out[3],
        query_out[4],
        forget_out[4],
        query_out[5],
        forget_out[5],
    )


def linear_pairs(fs_size, tp_size, target):
    pairs = []
    for f in range(fs_size):
        for t in range(tp_size):
            to_f, to_t = target(f, t)
            pairs.append((f * tp_size + t, to_f * tp_size + to_t))
    return pairs


def gather_operands(x_block, y_block, fs_size, tp_size):
    axes = ("fs", "tp")

    def move(value, target):
        return lax.ppermute(value, axes, linear_pairs(fs_size, tp_size, target))

    odd = lax.axis_index("tp") % 2 == 1

    def partner(f, t):
        return (f, t ^ 1)

    def first_hop(f, t):
        return (f ^ 1, t) if t % 2 == 0 else (f, t ^ 2)

    def second_hop(f, t):
        return (f, t ^ 2) if t % 2 == 0 else (f ^ 1, t)

    swapped = move(jnp.where(odd, x_block, y_block), partner)
    lane = jnp.stack([jnp.where(odd, swapped, x_block), jnp.where(odd, y_block, swapped)])
    lanes = [lane]
    for k in range(1, fs_size // 2):
        lanes.append(move(lane, lambda f, t, k=k: (f ^ (2 * k), t)))
    sets = []
    for lane in lanes:
        pair = jnp.stack([lane, move(lane, first_hop)])
        far = move(pair, second_hop)
        sets.append((pair, far, move(pair, partner), move(far, partner)))
    return sets


def tail_kernel(n_sets, place, *refs):
    pieces = [refs[4 * s : 4 * s + 4] for s in range(n_sets)]
    refs = refs[4 * n_sets :]
    sides = [refs[6 * i : 6 * i + 6] for i in range(2)]
    refs = refs[12:]
    outs = [refs[6 * i : 6 * i + 6] for i in range(2)]
    refs = refs[12:]
    x_all, y_all, grad, piece_sem, load_sem, store_sem = refs[:6]
    held = [refs[6 + 10 * i : 16 + 10 * i] for i in range(2)]
    odd, upper, band = place[0], place[1], place[2]
    tokens, width = pieces[0][0].shape[2:]
    model, total = grad.shape
    hidden = total // 2
    own = width // 2
    rows_here = held[0][0].shape[0]

    def piece_copies(s, x_pieces, y_pieces):
        for p in range(2):
            rows = pl.ds((2 * s + p) * tokens, tokens)
            for h in range(2):
                for c in range(2):
                    col = pl.multiple_of(((upper ^ h) * 2 + c) * width, width)
                    pltpu.make_async_copy(
                        x_pieces[h].at[p, c], x_all.at[rows, pl.ds(col, width)], piece_sem.at[0, s]
                    ).start()
                    for i in range(2):
                        pltpu.make_async_copy(
                            y_pieces[p].at[h, c, :, pl.ds(i * own, own)],
                            y_all.at[rows, pl.ds(i * hidden + (2 * h + c) * own, own)],
                            piece_sem.at[1, s],
                        ).start()

    for s in range(n_sets):
        pair, far, pair_other, far_other = pieces[s]

        @pl.when(odd == 0)
        def _():
            piece_copies(s, (pair, far), (pair_other, far_other))

        @pl.when(odd == 1)
        def _():
            piece_copies(s, (pair_other, far_other), (pair, far))

    loads = [
        [
            pltpu.make_async_copy(src, dst, load_sem.at[i, j])
            for j, (src, dst) in enumerate(zip(sides[i], held[i][:6], strict=True))
        ]
        for i in range(2)
    ]
    for side in loads:
        for copy in side:
            copy.start()
    for s in range(n_sets):
        for k, whole in enumerate((x_all, y_all)):
            rows = whole.at[pl.ds(2 * s * tokens, 2 * tokens)]
            pltpu.make_async_copy(rows, rows, piece_sem.at[k, s]).wait()

    step_rows = rows_here
    chunk = hidden // 2

    def product(m, squares):
        at = pl.multiple_of(m * step_rows, step_rows)
        x_part = x_all[:, pl.ds(at, step_rows)]
        squares = list(squares)
        for n in range(total // chunk):
            part = lax.dot_general(
                x_part,
                y_all[:, n * chunk : (n + 1) * chunk],
                (((0,), (0,)), ((), ())),
                preferred_element_type=jnp.float32,
            )
            grad[pl.ds(at, step_rows), n * chunk : (n + 1) * chunk] = part.astype(jnp.bfloat16)
            i = n * chunk // hidden
            squares[i] = squares[i] + jnp.sum((part * part).reshape(-1, 8, chunk), axis=0)
        return tuple(squares)

    zero = jnp.zeros((8, chunk), jnp.float32)
    squares = lax.fori_loop(0, model // step_rows, product, (zero, zero))

    stores = []
    first = pl.multiple_of(band * rows_here, rows_here)
    for i in range(2):
        rows, row_root, weight, moment, cols, col_root = held[i][:6]
        master_out, copy_out, step_out, moment_out = held[i][6:]
        for copy in loads[i]:
            copy.wait()
        square = jnp.sum(squares[i], keepdims=True)
        scale = jnp.sqrt(model * hidden / (square + 1.0))
        twice = scale * scale
        mine = pl.multiple_of(i * hidden + odd * own, own)
        band_grad = grad[pl.ds(first, rows_here), i * hidden : (i + 1) * hidden]
        row_factor = (1.0 - stat_decay) / hidden * twice

        def outer(n, carry):
            at = pl.multiple_of(n * rows_here, rows_here)
            part = lax.dot_general(
                band_grad,
                grad[pl.ds(at, rows_here), i * hidden : (i + 1) * hidden],
                (((1,), (1,)), ((), ())),
                preferred_element_type=jnp.float32,
            )
            rows[:, pl.ds(at, rows_here)] = (
                stat_decay * rows[:, pl.ds(at, rows_here)] + row_factor * part
            )
            return carry

        lax.fori_loop(0, model // rows_here, outer, 0)
        stores.append(pltpu.make_async_copy(rows, outs[i][4], store_sem.at[i, 4]))
        stores[-1].start()
        own_grad = grad[:, pl.ds(mine, own)]
        column_total = lax.dot_general(
            own_grad, own_grad, (((0,), (0,)), ((), ())), preferred_element_type=jnp.float32
        )
        left = jnp.dot(row_root[...], own_grad, preferred_element_type=jnp.float32)
        left_high = left.astype(jnp.bfloat16)
        left_low = (left - left_high.astype(jnp.float32)).astype(jnp.bfloat16)
        for h in range(own // HEAD):
            at = slice(h * HEAD, (h + 1) * HEAD)
            cols[h] = (
                stat_decay * cols[h]
                + (1.0 - stat_decay) / model * twice * column_total[at, at]
            )
            root = col_root[h]
            precond = scale * (
                jnp.dot(left_high[:, at], root, preferred_element_type=jnp.float32)
                + jnp.dot(left_low[:, at], root, preferred_element_type=jnp.float32)
            )
            moment_next = moment_decay * moment[:, at] + (1.0 - moment_decay) * precond
            update_step = moment_decay * moment_next + (1.0 - moment_decay) * precond
            master = weight[:, at] - learn_rate * update_step
            master_out[:, at] = master
            copy_out[:, at] = master.astype(jnp.bfloat16)
            step_out[:, at] = update_step
            moment_out[:, at] = moment_next
        for j, (src, dst) in enumerate(
            ((master_out, 0), (copy_out, 1), (step_out, 2), (moment_out, 3), (cols, 5))
        ):
            stores.append(pltpu.make_async_copy(src, outs[i][dst], store_sem.at[i, dst]))
            stores[-1].start()
    for copy in stores:
        copy.wait()


def gathered_plan(
    inputs,
    query_grad,
    forget_cot,
    query_weight,
    forget_weight,
    query_moment,
    forget_moment,
    query_rows,
    forget_rows,
    query_cols,
    forget_cols,
    query_row_root,
    forget_row_root,
    query_col_root,
    forget_col_root,
    fs_size,
    tp_size,
):
    sets = gather_operands(
        inputs, jnp.concatenate([query_grad, forget_cot], axis=1), fs_size, tp_size
    )
    tp_at = lax.axis_index("tp")
    place = jnp.stack([tp_at % 2, tp_at // 2, lax.axis_index("fs")]).astype(jnp.int32)
    tokens = inputs.shape[0] * fs_size
    model = inputs.shape[1] * tp_size
    total = 2 * query_grad.shape[1] * tp_size
    sides = (
        (query_rows, query_row_root, query_weight, query_moment, query_cols, query_col_root),
        (forget_rows, forget_row_root, forget_weight, forget_moment, forget_cols, forget_col_root),
    )
    wide = jax.ShapeDtypeStruct(query_weight.shape, jnp.float32)
    narrow = jax.ShapeDtypeStruct(query_weight.shape, jnp.bfloat16)
    row_kind = jax.ShapeDtypeStruct(query_rows.shape, jnp.float32)
    col_kind = jax.ShapeDtypeStruct(query_cols.shape, jnp.float32)
    kinds = (wide, narrow, wide, wide, row_kind, col_kind)
    held = []
    for side in sides:
        held += [pltpu.VMEM(v.shape, v.dtype) for v in side]
        held += [pltpu.VMEM(k.shape, k.dtype) for k in kinds[:4]]
    operands = [v for pieces in sets for v in pieces] + [v for side in sides for v in side]
    anywhere = pl.BlockSpec(memory_space=pl.ANY)
    out = pl.pallas_call(
        partial(tail_kernel, len(sets)),
        out_shape=kinds * 2,
        in_specs=[pl.BlockSpec(memory_space=pltpu.SMEM)] + [anywhere] * len(operands),
        out_specs=[anywhere] * 12,
        scratch_shapes=[
            pltpu.VMEM((tokens, model), jnp.bfloat16),
            pltpu.VMEM((tokens, total), jnp.bfloat16),
            pltpu.VMEM((model, total), jnp.bfloat16),
            pltpu.SemaphoreType.DMA((2, len(sets))),
            pltpu.SemaphoreType.DMA((2, 6)),
            pltpu.SemaphoreType.DMA((2, 6)),
        ]
        + held,
        compiler_params=pltpu.CompilerParams(vmem_limit_bytes=48 * 2**20),
        name="tail",
    )(place, *operands)
    return tuple(v for both in zip(out[:6], out[6:], strict=True) for v in both)


def use_gathered(tokens, model, hidden, fs_size, tp_size):
    blocks = fs_size // 2
    square_grid = tp_size == 4 and fs_size % 2 == 0 and blocks & (blocks - 1) == 0
    return square_grid and tokens * (model + 2 * hidden) <= model * 2 * hidden


def on_device(fs_size, tp_size, inputs, query_grad, forget_grad, forget_pre, lower_bound, *rest):
    sigma_gate = jax.nn.sigmoid(forget_pre.astype(jnp.float32))
    forget_cot = (
        forget_grad.astype(jnp.float32) * (1.0 - lower_bound) * sigma_gate * (1.0 - sigma_gate)
    ).astype(jnp.bfloat16)
    tokens = inputs.shape[0] * fs_size
    if use_gathered(tokens, inputs.shape[1] * tp_size, query_grad.shape[1] * tp_size, fs_size, tp_size):
        return gathered_plan(inputs, query_grad, forget_cot, *rest, fs_size, tp_size)
    return summed_plan(inputs, query_grad, forget_cot, *rest)


def solution(mesh):
    in_specs = (
        P("fs", "tp"),
        P("fs", "tp"),
        P("fs", "tp"),
        P("fs", "tp"),
        P("tp"),
        P("fs", "tp"),
        P("fs", "tp"),
        P("fs", "tp"),
        P("fs", "tp"),
        P("fs", None),
        P("fs", None),
        P("tp", None, None),
        P("tp", None, None),
        P("fs", None),
        P("fs", None),
        P("tp", None, None),
        P("tp", None, None),
    )
    out_specs = (
        P("fs", "tp"),
        P("fs", "tp"),
        P("fs", "tp"),
        P("fs", "tp"),
        P("fs", "tp"),
        P("fs", "tp"),
        P("fs", "tp"),
        P("fs", "tp"),
        P("fs", None),
        P("fs", None),
        P("tp", None, None),
        P("tp", None, None),
    )
    sizes = (mesh.shape["fs"], mesh.shape["tp"])
    return jax.shard_map(
        partial(on_device, *sizes), mesh=mesh, in_specs=in_specs, out_specs=out_specs, check_vma=False
    )
```

```python
from functools import partial

import jax
import jax.numpy as jnp
from jax import lax
from jax.experimental import pallas as pl
from jax.experimental.pallas import tpu as pltpu
from jax.sharding import PartitionSpec as P


D = 2048
HW = 1024
HEAD = 128


stat_decay = 0.9
moment_decay = 0.9
learn_rate = 0.02
highest = lax.Precision.HIGHEST


def fold_one(carry_state, shard_piece, offset, root_mine, grad_mine):
    left_sum, outer_rows, column_total = carry_state
    row_count, col_width = shard_piece.shape
    left_sum = left_sum + jnp.dot(root_mine, shard_piece, precision=highest)
    outer_piece = lax.dot_general(
        grad_mine, shard_piece, (((1,), (1,)), ((), ())), precision=highest
    )
    outer_rows = lax.dynamic_update_slice_in_dim(outer_rows, outer_piece, offset, 1)
    by_head = shard_piece.reshape(row_count, col_width // HEAD, HEAD)
    column_total = column_total + jnp.einsum("rhi,rhj->hij", by_head, by_head, precision=highest)
    return (left_sum, outer_rows, column_total)


def finish(weight, moment, rows, cols, col_root, left_sum, outer_rows, column_total, square):
    norm_scale = jnp.sqrt(D * HW / (square + 1.0))
    scale_twice = norm_scale * norm_scale
    rows_next = stat_decay * rows + (1.0 - stat_decay) / HW * scale_twice * outer_rows
    cols_next = stat_decay * cols + (1.0 - stat_decay) / D * scale_twice * column_total
    shard_rows, col_width = left_sum.shape
    shaped = left_sum.reshape(shard_rows, col_width // HEAD, HEAD)
    precond = norm_scale * jnp.einsum(
        "rhi,hij->rhj", shaped, col_root.astype(jnp.float32), precision=highest
    ).reshape(shard_rows, col_width)
    moment_next = moment_decay * moment + (1.0 - moment_decay) * precond
    update_step = moment_decay * moment_next + (1.0 - moment_decay) * precond
    master = weight - learn_rate * update_step
    return (master, master.astype(jnp.bfloat16), update_step, moment_next, rows_next, cols_next)


def summed_plan(
    inputs,
    query_grad,
    forget_cot,
    query_weight,
    forget_weight,
    query_moment,
    forget_moment,
    query_rows,
    forget_rows,
    query_cols,
    forget_cols,
    query_row_root,
    forget_row_root,
    query_col_root,
    forget_col_root,
):
    gathered = lax.all_gather(inputs, "tp", axis=1, tiled=True)
    shard_rows, col_width = query_weight.shape
    heads_here = col_width // HEAD
    row_roots = (query_row_root.astype(jnp.float32), forget_row_root.astype(jnp.float32))
    empty = (
        jnp.zeros((shard_rows, col_width), jnp.float32),
        jnp.zeros((shard_rows, D), jnp.float32),
        jnp.zeros((heads_here, HEAD, HEAD), jnp.float32),
    )
    joined = jnp.concatenate([query_grad, forget_cot], axis=1)
    summed = lax.psum_scatter(
        lax.dot_general(
            gathered, joined, (((0,), (0,)), ((), ())), preferred_element_type=jnp.float32
        ),
        "fs",
        scatter_dimension=0,
        tiled=True,
    )
    gradients = (summed[:, :col_width], summed[:, col_width:])
    offset = jnp.int32(0)
    results = (
        fold_one(
            empty,
            lax.all_gather(gradients[0].astype(jnp.bfloat16), "fs", axis=0, tiled=True).astype(
                jnp.float32
            ),
            offset,
            row_roots[0],
            gradients[0],
        ),
        fold_one(
            empty,
            lax.all_gather(gradients[1].astype(jnp.bfloat16), "fs", axis=0, tiled=True).astype(
                jnp.float32
            ),
            offset,
            row_roots[1],
            gradients[1],
        ),
    )
    query_trace = jnp.sum(jnp.diagonal(results[0][2], axis1=1, axis2=2))
    forget_trace = jnp.sum(jnp.diagonal(results[1][2], axis1=1, axis2=2))
    query_outer, forget_outer, query_square, forget_square = (
        lax.psum(results[0][1].astype(jnp.bfloat16), "tp").astype(jnp.float32),
        lax.psum(results[1][1].astype(jnp.bfloat16), "tp").astype(jnp.float32),
        lax.psum(query_trace.astype(jnp.bfloat16), "tp").astype(jnp.float32),
        lax.psum(forget_trace.astype(jnp.bfloat16), "tp").astype(jnp.float32),
    )
    query_out = finish(
        query_weight,
        query_moment,
        query_rows,
        query_cols,
        query_col_root,
        results[0][0],
        query_outer,
        results[0][2],
        query_square,
    )
    forget_out = finish(
        forget_weight,
        forget_moment,
        forget_rows,
        forget_cols,
        forget_col_root,
        results[1][0],
        forget_outer,
        results[1][2],
        forget_square,
    )
    return (
        query_out[0],
        forget_out[0],
        query_out[1],
        forget_out[1],
        query_out[2],
        forget_out[2],
        query_out[3],
        forget_out[3],
        query_out[4],
        forget_out[4],
        query_out[5],
        forget_out[5],
    )


def linear_pairs(fs_size, tp_size, target):
    pairs = []
    for f in range(fs_size):
        for t in range(tp_size):
            to_f, to_t = target(f, t)
            pairs.append((f * tp_size + t, to_f * tp_size + to_t))
    return pairs


def gather_operands(x_block, y_block, fs_size, tp_size):
    axes = ("fs", "tp")

    def move(value, target):
        return lax.ppermute(value, axes, linear_pairs(fs_size, tp_size, target))

    odd = lax.axis_index("tp") % 2 == 1

    def partner(f, t):
        return (f, t ^ 1)

    def first_hop(f, t):
        return (f ^ 1, t) if t % 2 == 0 else (f, t ^ 2)

    def second_hop(f, t):
        return (f, t ^ 2) if t % 2 == 0 else (f ^ 1, t)

    swapped = move(jnp.where(odd, x_block, y_block), partner)
    lanes = [jnp.stack([jnp.where(odd, swapped, x_block), jnp.where(odd, y_block, swapped)])]
    for k in range(1, fs_size // 2):
        step = k & -k if k & (k - 1) == 0 else k & (k - 1) ^ k
        source = lanes[k ^ step]
        lanes.append(move(source, lambda f, t, step=step: (f ^ (2 * step), t)))
    sets = []
    for lane in lanes:
        pair = jnp.stack([lane, move(lane, first_hop)])
        far = move(pair, second_hop)
        sets.append((pair, far, move(pair, partner), move(far, partner)))
    return sets


def assemble(place, pieces, x_set, y_set, sem):
    odd, upper = place[0], place[1]
    tokens, width = pieces[0].shape[2:]
    own = width // 2
    hidden = y_set.shape[1] // 2

    def copies(x_pieces, y_pieces):
        for p in range(2):
            rows = pl.ds(p * tokens, tokens)
            for h in range(2):
                for c in range(2):
                    col = pl.multiple_of(((upper ^ h) * 2 + c) * width, width)
                    pltpu.make_async_copy(
                        x_pieces[h].at[p, c], x_set.at[rows, pl.ds(col, width)], sem.at[0]
                    ).start()
                    for i in range(2):
                        pltpu.make_async_copy(
                            y_pieces[p].at[h, c, :, pl.ds(i * own, own)],
                            y_set.at[rows, pl.ds(i * hidden + (2 * h + c) * own, own)],
                            sem.at[1],
                        ).start()

    pair, far, pair_other, far_other = pieces

    @pl.when(odd == 0)
    def _():
        copies((pair, far), (pair_other, far_other))

    @pl.when(odd == 1)
    def _():
        copies((pair_other, far_other), (pair, far))


def assembled(x_set, y_set, sem):
    for k, whole in enumerate((x_set, y_set)):
        pltpu.make_async_copy(whole, whole, sem.at[k]).wait()


def chunk_product(x_set, y_set, m, n, rows, chunk):
    at = pl.multiple_of(m * rows, rows)
    return lax.dot_general(
        x_set[:, pl.ds(at, rows)],
        y_set[:, n * chunk : (n + 1) * chunk],
        (((0,), (0,)), ((), ())),
        preferred_element_type=jnp.float32,
    )


def sum_kernel(first, place, *refs):
    pieces, refs = refs[:4], refs[4:]
    if not first:
        refs = refs[1:]
    acc, x_set, y_set, sem = refs
    assemble(place, pieces, x_set, y_set, sem)
    assembled(x_set, y_set, sem)
    model, total = acc.shape
    rows = pieces[0].shape[3] // 2
    chunk = total // 4

    def product(m, carry):
        at = pl.multiple_of(m * rows, rows)
        for n in range(total // chunk):
            cols = slice(n * chunk, (n + 1) * chunk)
            part = chunk_product(x_set, y_set, m, n, rows, chunk)
            acc[pl.ds(at, rows), cols] = part if first else acc[pl.ds(at, rows), cols] + part
        return carry

    lax.fori_loop(0, model // rows, product, 0)


def tail_kernel(place, *refs):
    pieces, acc, refs = refs[:4], refs[4], refs[5:]
    sides = [refs[6 * i : 6 * i + 6] for i in range(2)]
    refs = refs[12:]
    outs = [refs[6 * i : 6 * i + 6] for i in range(2)]
    refs = refs[12:]
    x_set, y_set, grad, sem, load_sem, store_sem = refs[:6]
    held = [refs[6 + 10 * i : 16 + 10 * i] for i in range(2)]
    odd, band = place[0], place[2]
    model, total = grad.shape
    hidden = total // 2
    own = pieces[0].shape[3] // 2
    rows_here = held[0][0].shape[0]

    assemble(place, pieces, x_set, y_set, sem)
    loads = [
        [
            pltpu.make_async_copy(src, dst, load_sem.at[i, j])
            for j, (src, dst) in enumerate(zip(sides[i], held[i][:6], strict=True))
        ]
        for i in range(2)
    ]
    for side in loads:
        for copy in side:
            copy.start()
    assembled(x_set, y_set, sem)

    chunk = hidden // 2

    def product(m, squares):
        at = pl.multiple_of(m * rows_here, rows_here)
        squares = list(squares)
        for n in range(total // chunk):
            cols = slice(n * chunk, (n + 1) * chunk)
            part = acc[pl.ds(at, rows_here), cols] + chunk_product(
                x_set, y_set, m, n, rows_here, chunk
            )
            grad[pl.ds(at, rows_here), cols] = part.astype(jnp.bfloat16)
            i = n * chunk // hidden
            squares[i] = squares[i] + jnp.sum((part * part).reshape(-1, 8, chunk), axis=0)
        return tuple(squares)

    zero = jnp.zeros((8, chunk), jnp.float32)
    squares = lax.fori_loop(0, model // rows_here, product, (zero, zero))

    stores = []
    first = pl.multiple_of(band * rows_here, rows_here)
    for i in range(2):
        rows, row_root, weight, moment, cols, col_root = held[i][:6]
        master_out, copy_out, step_out, moment_out = held[i][6:]
        for copy in loads[i]:
            copy.wait()
        square = jnp.sum(squares[i], keepdims=True)
        scale = jnp.sqrt(model * hidden / (square + 1.0))
        twice = scale * scale
        mine = pl.multiple_of(i * hidden + odd * own, own)
        band_grad = grad[pl.ds(first, rows_here), i * hidden : (i + 1) * hidden]
        row_factor = (1.0 - stat_decay) / hidden * twice

        def outer(n, carry):
            at = pl.multiple_of(n * rows_here, rows_here)
            part = lax.dot_general(
                band_grad,
                grad[pl.ds(at, rows_here), i * hidden : (i + 1) * hidden],
                (((1,), (1,)), ((), ())),
                preferred_element_type=jnp.float32,
            )
            rows[:, pl.ds(at, rows_here)] = (
                stat_decay * rows[:, pl.ds(at, rows_here)] + row_factor * part
            )
            return carry

        lax.fori_loop(0, model // rows_here, outer, 0)
        stores.append(pltpu.make_async_copy(rows, outs[i][4], store_sem.at[i, 4]))
        stores[-1].start()
        own_grad = grad[:, pl.ds(mine, own)]
        column_total = lax.dot_general(
            own_grad, own_grad, (((0,), (0,)), ((), ())), preferred_element_type=jnp.float32
        )
        left = jnp.dot(row_root[...], own_grad, preferred_element_type=jnp.float32)
        left_high = left.astype(jnp.bfloat16)
        left_low = (left - left_high.astype(jnp.float32)).astype(jnp.bfloat16)
        for h in range(own // HEAD):
            at = slice(h * HEAD, (h + 1) * HEAD)
            cols[h] = (
                stat_decay * cols[h]
                + (1.0 - stat_decay) / model * twice * column_total[at, at]
            )
            root = col_root[h]
            precond = scale * (
                jnp.dot(left_high[:, at], root, preferred_element_type=jnp.float32)
                + jnp.dot(left_low[:, at], root, preferred_element_type=jnp.float32)
            )
            moment_next = moment_decay * moment[:, at] + (1.0 - moment_decay) * precond
            update_step = moment_decay * moment_next + (1.0 - moment_decay) * precond
            master = weight[:, at] - learn_rate * update_step
            master_out[:, at] = master
            copy_out[:, at] = master.astype(jnp.bfloat16)
            step_out[:, at] = update_step
            moment_out[:, at] = moment_next
        for src, dst in ((master_out, 0), (copy_out, 1), (step_out, 2), (moment_out, 3), (cols, 5)):
            stores.append(pltpu.make_async_copy(src, outs[i][dst], store_sem.at[i, dst]))
            stores[-1].start()
    for copy in stores:
        copy.wait()


def gathered_plan(
    inputs,
    query_grad,
    forget_cot,
    query_weight,
    forget_weight,
    query_moment,
    forget_moment,
    query_rows,
    forget_rows,
    query_cols,
    forget_cols,
    query_row_root,
    forget_row_root,
    query_col_root,
    forget_col_root,
    fs_size,
    tp_size,
):
    sets = gather_operands(
        inputs, jnp.concatenate([query_grad, forget_cot], axis=1), fs_size, tp_size
    )
    tp_at = lax.axis_index("tp")
    place = jnp.stack([tp_at % 2, tp_at // 2, lax.axis_index("fs")]).astype(jnp.int32)
    model = inputs.shape[1] * tp_size
    total = 2 * query_grad.shape[1] * tp_size
    sides = (
        (query_rows, query_row_root, query_weight, query_moment, query_cols, query_col_root),
        (forget_rows, forget_row_root, forget_weight, forget_moment, forget_cols, forget_col_root),
    )
    wide = jax.ShapeDtypeStruct(query_weight.shape, jnp.float32)
    narrow = jax.ShapeDtypeStruct(query_weight.shape, jnp.bfloat16)
    row_kind = jax.ShapeDtypeStruct(query_rows.shape, jnp.float32)
    col_kind = jax.ShapeDtypeStruct(query_cols.shape, jnp.float32)
    kinds = (wide, narrow, wide, wide, row_kind, col_kind)
    held = []
    for side in sides:
        held += [pltpu.VMEM(v.shape, v.dtype) for v in side]
        held += [pltpu.VMEM(k.shape, k.dtype) for k in kinds[:4]]
    anywhere = pl.BlockSpec(memory_space=pl.ANY)
    hbm = pl.BlockSpec(memory_space=pltpu.HBM)
    vmem = pl.BlockSpec(memory_space=pltpu.VMEM)
    smem = pl.BlockSpec(memory_space=pltpu.SMEM)
    set_scratch = [
        pltpu.VMEM((2 * inputs.shape[0], model), jnp.bfloat16),
        pltpu.VMEM((2 * inputs.shape[0], total), jnp.bfloat16),
    ]
    params = pltpu.CompilerParams(vmem_limit_bytes=26 * 2**20)
    acc = []
    for pieces in sets[:-1]:
        acc = [
            pl.pallas_call(
                partial(sum_kernel, not acc),
                out_shape=pltpu.VMEM((model, total), jnp.float32),
                in_specs=[smem] + [anywhere] * 4 + [vmem] * len(acc),
                out_specs=vmem,
                scratch_shapes=set_scratch + [pltpu.SemaphoreType.DMA((2,))],
                input_output_aliases={5: 0} if acc else {},
                compiler_params=params,
            )(place, *pieces, *acc)
        ]
    operands = [*sets[-1], pltpu.with_memory_space_constraint(*acc, pltpu.VMEM)]
    operands += [pltpu.with_memory_space_constraint(v, pltpu.HBM) for side in sides for v in side]
    out = pl.pallas_call(
        tail_kernel,
        out_shape=kinds * 2,
        in_specs=[smem] + [anywhere] * 4 + [vmem] + [hbm] * 12,
        out_specs=[hbm] * 12,
        scratch_shapes=set_scratch
        + [
            pltpu.VMEM((model, total), jnp.bfloat16),
            pltpu.SemaphoreType.DMA((2,)),
            pltpu.SemaphoreType.DMA((2, 6)),
            pltpu.SemaphoreType.DMA((2, 6)),
        ]
        + held,
        compiler_params=params,
        name="tail",
    )(place, *operands)
    return tuple(v for both in zip(out[:6], out[6:], strict=True) for v in both)


def use_gathered(tokens, model, hidden, fs_size, tp_size):
    blocks = fs_size // 2
    square_grid = tp_size == 4 and fs_size % 2 == 0 and blocks & (blocks - 1) == 0
    return square_grid and tokens * (model + 2 * hidden) <= model * 2 * hidden


def on_device(fs_size, tp_size, inputs, query_grad, forget_grad, forget_pre, lower_bound, *rest):
    sigma_gate = jax.nn.sigmoid(forget_pre.astype(jnp.float32))
    forget_cot = (
        forget_grad.astype(jnp.float32) * (1.0 - lower_bound) * sigma_gate * (1.0 - sigma_gate)
    ).astype(jnp.bfloat16)
    tokens = inputs.shape[0] * fs_size
    if use_gathered(tokens, inputs.shape[1] * tp_size, query_grad.shape[1] * tp_size, fs_size, tp_size):
        return gathered_plan(inputs, query_grad, forget_cot, *rest, fs_size, tp_size)
    return summed_plan(inputs, query_grad, forget_cot, *rest)


def solution(mesh):
    in_specs = (
        P("fs", "tp"),
        P("fs", "tp"),
        P("fs", "tp"),
        P("fs", "tp"),
        P("tp"),
        P("fs", "tp"),
        P("fs", "tp"),
        P("fs", "tp"),
        P("fs", "tp"),
        P("fs", None),
        P("fs", None),
        P("tp", None, None),
        P("tp", None, None),
        P("fs", None),
        P("fs", None),
        P("tp", None, None),
        P("tp", None, None),
    )
    out_specs = (
        P("fs", "tp"),
        P("fs", "tp"),
        P("fs", "tp"),
        P("fs", "tp"),
        P("fs", "tp"),
        P("fs", "tp"),
        P("fs", "tp"),
        P("fs", "tp"),
        P("fs", None),
        P("fs", None),
        P("tp", None, None),
        P("tp", None, None),
    )
    sizes = (mesh.shape["fs"], mesh.shape["tp"])
    return jax.shard_map(
        partial(on_device, *sizes), mesh=mesh, in_specs=in_specs, out_specs=out_specs, check_vma=False
    )
```

```python
from functools import partial

import jax
import jax.numpy as jnp
from jax import lax
from jax.experimental import pallas as pl
from jax.experimental.pallas import tpu as pltpu
from jax.sharding import PartitionSpec as P


D = 2048
HW = 1024
HEAD = 128


stat_decay = 0.9
moment_decay = 0.9
learn_rate = 0.02
highest = lax.Precision.HIGHEST


def fold_one(carry_state, shard_piece, offset, root_mine, grad_mine):
    left_sum, outer_rows, column_total = carry_state
    row_count, col_width = shard_piece.shape
    left_sum = left_sum + jnp.dot(root_mine, shard_piece, precision=highest)
    outer_piece = lax.dot_general(
        grad_mine, shard_piece, (((1,), (1,)), ((), ())), precision=highest
    )
    outer_rows = lax.dynamic_update_slice_in_dim(outer_rows, outer_piece, offset, 1)
    by_head = shard_piece.reshape(row_count, col_width // HEAD, HEAD)
    column_total = column_total + jnp.einsum("rhi,rhj->hij", by_head, by_head, precision=highest)
    return (left_sum, outer_rows, column_total)


def finish(weight, moment, rows, cols, col_root, left_sum, outer_rows, column_total, square):
    norm_scale = jnp.sqrt(D * HW / (square + 1.0))
    scale_twice = norm_scale * norm_scale
    rows_next = stat_decay * rows + (1.0 - stat_decay) / HW * scale_twice * outer_rows
    cols_next = stat_decay * cols + (1.0 - stat_decay) / D * scale_twice * column_total
    shard_rows, col_width = left_sum.shape
    shaped = left_sum.reshape(shard_rows, col_width // HEAD, HEAD)
    precond = norm_scale * jnp.einsum(
        "rhi,hij->rhj", shaped, col_root.astype(jnp.float32), precision=highest
    ).reshape(shard_rows, col_width)
    moment_next = moment_decay * moment + (1.0 - moment_decay) * precond
    update_step = moment_decay * moment_next + (1.0 - moment_decay) * precond
    master = weight - learn_rate * update_step
    return (master, master.astype(jnp.bfloat16), update_step, moment_next, rows_next, cols_next)


def summed_plan(
    inputs,
    query_grad,
    forget_cot,
    query_weight,
    forget_weight,
    query_moment,
    forget_moment,
    query_rows,
    forget_rows,
    query_cols,
    forget_cols,
    query_row_root,
    forget_row_root,
    query_col_root,
    forget_col_root,
):
    gathered = lax.all_gather(inputs, "tp", axis=1, tiled=True)
    shard_rows, col_width = query_weight.shape
    heads_here = col_width // HEAD
    row_roots = (query_row_root.astype(jnp.float32), forget_row_root.astype(jnp.float32))
    empty = (
        jnp.zeros((shard_rows, col_width), jnp.float32),
        jnp.zeros((shard_rows, D), jnp.float32),
        jnp.zeros((heads_here, HEAD, HEAD), jnp.float32),
    )
    joined = jnp.concatenate([query_grad, forget_cot], axis=1)
    summed = lax.psum_scatter(
        lax.dot_general(
            gathered, joined, (((0,), (0,)), ((), ())), preferred_element_type=jnp.float32
        ),
        "fs",
        scatter_dimension=0,
        tiled=True,
    )
    gradients = (summed[:, :col_width], summed[:, col_width:])
    offset = jnp.int32(0)
    results = (
        fold_one(
            empty,
            lax.all_gather(gradients[0].astype(jnp.bfloat16), "fs", axis=0, tiled=True).astype(
                jnp.float32
            ),
            offset,
            row_roots[0],
            gradients[0],
        ),
        fold_one(
            empty,
            lax.all_gather(gradients[1].astype(jnp.bfloat16), "fs", axis=0, tiled=True).astype(
                jnp.float32
            ),
            offset,
            row_roots[1],
            gradients[1],
        ),
    )
    query_trace = jnp.sum(jnp.diagonal(results[0][2], axis1=1, axis2=2))
    forget_trace = jnp.sum(jnp.diagonal(results[1][2], axis1=1, axis2=2))
    query_outer, forget_outer, query_square, forget_square = (
        lax.psum(results[0][1].astype(jnp.bfloat16), "tp").astype(jnp.float32),
        lax.psum(results[1][1].astype(jnp.bfloat16), "tp").astype(jnp.float32),
        lax.psum(query_trace.astype(jnp.bfloat16), "tp").astype(jnp.float32),
        lax.psum(forget_trace.astype(jnp.bfloat16), "tp").astype(jnp.float32),
    )
    query_out = finish(
        query_weight,
        query_moment,
        query_rows,
        query_cols,
        query_col_root,
        results[0][0],
        query_outer,
        results[0][2],
        query_square,
    )
    forget_out = finish(
        forget_weight,
        forget_moment,
        forget_rows,
        forget_cols,
        forget_col_root,
        results[1][0],
        forget_outer,
        results[1][2],
        forget_square,
    )
    return (
        query_out[0],
        forget_out[0],
        query_out[1],
        forget_out[1],
        query_out[2],
        forget_out[2],
        query_out[3],
        forget_out[3],
        query_out[4],
        forget_out[4],
        query_out[5],
        forget_out[5],
    )


def linear_pairs(fs_size, tp_size, target):
    pairs = []
    for f in range(fs_size):
        for t in range(tp_size):
            to_f, to_t = target(f, t)
            pairs.append((f * tp_size + t, to_f * tp_size + to_t))
    return pairs


def gather_operands(keep, send, fs_size, tp_size):
    axes = ("fs", "tp")

    def move(value, target):
        return lax.ppermute(value, axes, linear_pairs(fs_size, tp_size, target))

    def partner(f, t):
        return (f, t ^ 1)

    def first_hop(f, t):
        return (f ^ 1, t) if t % 2 == 0 else (f, t ^ 2)

    def second_hop(f, t):
        return (f, t ^ 2) if t % 2 == 0 else (f ^ 1, t)

    lanes = [jnp.stack([keep, move(send, partner)])]
    for k in range(1, fs_size // 2):
        step = k & -k if k & (k - 1) == 0 else k & (k - 1) ^ k
        source = lanes[k ^ step]
        lanes.append(move(source, lambda f, t, step=step: (f ^ (2 * step), t)))
    sets = []
    for lane in lanes:
        pair = jnp.stack([lane, move(lane, first_hop)])
        far = move(pair, second_hop)
        sets.append((pair, far, move(pair, partner), move(far, partner)))
    return sets


def assemble(place, pieces, x_set, y_set, sem):
    odd, upper = place[0], place[1]
    tokens, width = pieces[0].shape[2:]
    own = width // 2
    hidden = y_set.shape[1] // 2

    def copies(x_pieces, y_pieces):
        for p in range(2):
            rows = pl.ds(p * tokens, tokens)
            for h in range(2):
                for c in range(2):
                    col = pl.multiple_of(((upper ^ h) * 2 + c) * width, width)
                    pltpu.make_async_copy(
                        x_pieces[h].at[p, c], x_set.at[rows, pl.ds(col, width)], sem.at[0]
                    ).start()
                    for i in range(2):
                        pltpu.make_async_copy(
                            y_pieces[p].at[h, 1 - c, :, pl.ds(i * own, own)],
                            y_set.at[rows, pl.ds(i * hidden + (2 * h + c) * own, own)],
                            sem.at[1],
                        ).start()

    pair, far, pair_other, far_other = pieces

    @pl.when(odd == 0)
    def _():
        copies((pair, far), (pair_other, far_other))

    @pl.when(odd == 1)
    def _():
        copies((pair_other, far_other), (pair, far))


def assembled(x_set, y_set, sem):
    for k, whole in enumerate((x_set, y_set)):
        pltpu.make_async_copy(whole, whole, sem.at[k]).wait()


def product(x_set, y_set, cols):
    return lax.dot_general(
        x_set[...], y_set[:, cols], (((0,), (0,)), ((), ())), preferred_element_type=jnp.float32
    )


def sum_kernel(first, place, *refs):
    pieces, refs = refs[:4], refs[4:]
    if not first:
        refs = refs[1:]
    acc, x_set, y_set, sem = refs
    assemble(place, pieces, x_set, y_set, sem)
    assembled(x_set, y_set, sem)
    total, chunk = acc.shape[1], x_set.shape[0]
    for at in range(0, total, chunk):
        cols = slice(at, at + chunk)
        part = product(x_set, y_set, cols)
        acc[:, cols] = part if first else acc[:, cols] + part


def tail_kernel(place, *refs):
    pieces, acc, refs = refs[:4], refs[4], refs[5:]
    sides = [refs[6 * i : 6 * i + 6] for i in range(2)]
    refs = refs[12:]
    outs = [refs[6 * i : 6 * i + 6] for i in range(2)]
    refs = refs[12:]
    x_set, y_set, grad, sem, load_sem, store_sem = refs[:6]
    held = [refs[6 + 10 * i : 16 + 10 * i] for i in range(2)]
    odd, band = place[0], place[2]
    model, total = grad.shape
    hidden = total // 2
    own = pieces[0].shape[3] // 2
    rows_here = held[0][0].shape[0]

    assemble(place, pieces, x_set, y_set, sem)
    loads = [
        [
            pltpu.make_async_copy(src, dst, load_sem.at[i, j])
            for j, (src, dst) in enumerate(zip(sides[i], held[i][:6], strict=True))
        ]
        for i in range(2)
    ]
    for side in loads:
        for copy in side:
            copy.start()
    assembled(x_set, y_set, sem)

    chunk = x_set.shape[0]
    squares = [jnp.zeros((8, chunk), jnp.float32)] * 2
    for at in range(0, total, chunk):
        cols = slice(at, at + chunk)
        part = acc[:, cols] + product(x_set, y_set, cols)
        grad[:, cols] = part.astype(jnp.bfloat16)
        squares[at // hidden] += jnp.sum((part * part).reshape(-1, 8, chunk), axis=0)

    stores = []
    first = pl.multiple_of(band * rows_here, rows_here)
    for i in range(2):
        rows, row_root, weight, moment, cols, col_root = held[i][:6]
        master_out, copy_out, step_out, moment_out = held[i][6:]
        for copy in loads[i]:
            copy.wait()
        square = jnp.sum(squares[i], keepdims=True)
        scale = jnp.sqrt(model * hidden / (square + 1.0))
        twice = scale * scale
        mine = pl.multiple_of(i * hidden + odd * own, own)
        band_grad = grad[pl.ds(first, rows_here), i * hidden : (i + 1) * hidden]
        row_factor = (1.0 - stat_decay) / hidden * twice

        for at in range(0, model, own * 2):
            part = lax.dot_general(
                band_grad,
                grad[at : at + own * 2, i * hidden : (i + 1) * hidden],
                (((1,), (1,)), ((), ())),
                preferred_element_type=jnp.float32,
            )
            to = slice(at, at + own * 2)
            rows[:, to] = stat_decay * rows[:, to] + row_factor * part
        stores.append(pltpu.make_async_copy(rows, outs[i][4], store_sem.at[i, 4]))
        stores[-1].start()
        own_grad = grad[:, pl.ds(mine, own)]
        column_total = lax.dot_general(
            own_grad, own_grad, (((0,), (0,)), ((), ())), preferred_element_type=jnp.float32
        )
        left = jnp.dot(row_root[...], own_grad, preferred_element_type=jnp.float32)
        left_high = left.astype(jnp.bfloat16)
        left_low = (left - left_high.astype(jnp.float32)).astype(jnp.bfloat16)
        for h in range(own // HEAD):
            at = slice(h * HEAD, (h + 1) * HEAD)
            cols[h] = (
                stat_decay * cols[h]
                + (1.0 - stat_decay) / model * twice * column_total[at, at]
            )
            root = col_root[h]
            precond = scale * (
                jnp.dot(left_high[:, at], root, preferred_element_type=jnp.float32)
                + jnp.dot(left_low[:, at], root, preferred_element_type=jnp.float32)
            )
            moment_next = moment_decay * moment[:, at] + (1.0 - moment_decay) * precond
            update_step = moment_decay * moment_next + (1.0 - moment_decay) * precond
            master = weight[:, at] - learn_rate * update_step
            master_out[:, at] = master
            copy_out[:, at] = master.astype(jnp.bfloat16)
            step_out[:, at] = update_step
            moment_out[:, at] = moment_next
        for src, dst in ((master_out, 0), (copy_out, 1), (step_out, 2), (moment_out, 3), (cols, 5)):
            stores.append(pltpu.make_async_copy(src, outs[i][dst], store_sem.at[i, dst]))
            stores[-1].start()
    for copy in stores:
        copy.wait()


def prepare_kernel(place, *refs):
    sources, (keep, send), held, sem = refs[:5], refs[5:7], refs[7:12], refs[12]
    copies = [
        pltpu.make_async_copy(src, dst, sem.at[j])
        for j, (src, dst) in enumerate(zip(sources, held, strict=True))
    ]
    for copy in copies:
        copy.start()
    for copy in copies:
        copy.wait()
    inputs, query_grad, forget_grad, forget_pre, lower_bound = held
    own = query_grad.shape[1]
    sigma_gate = jax.nn.sigmoid(forget_pre[...].astype(jnp.float32))
    forget_cot = (
        forget_grad[...].astype(jnp.float32)
        * (1.0 - lower_bound[...])
        * sigma_gate
        * (1.0 - sigma_gate)
    ).astype(jnp.bfloat16)

    def write(x_to, y_to):
        x_to[...] = inputs[...]
        y_to[:, :own] = query_grad[...]
        y_to[:, own:] = forget_cot

    @pl.when(place[0] == 0)
    def _():
        write(keep, send)

    @pl.when(place[0] == 1)
    def _():
        write(send, keep)


def gathered_plan(
    inputs,
    query_grad,
    forget_grad,
    forget_pre,
    lower_bound,
    query_weight,
    forget_weight,
    query_moment,
    forget_moment,
    query_rows,
    forget_rows,
    query_cols,
    forget_cols,
    query_row_root,
    forget_row_root,
    query_col_root,
    forget_col_root,
    fs_size,
    tp_size,
):
    tp_at = lax.axis_index("tp")
    place = jnp.stack([tp_at & 1, tp_at >> 1, lax.axis_index("fs")]).astype(jnp.int32)
    smem = pl.BlockSpec(memory_space=pltpu.SMEM)
    vmem = pl.BlockSpec(memory_space=pltpu.VMEM)
    params = pltpu.CompilerParams(vmem_limit_bytes=26 * 2**20)
    hbm = pl.BlockSpec(memory_space=pltpu.HBM)
    saved = (inputs, query_grad, forget_grad, forget_pre, lower_bound[None])
    keep, send = pl.pallas_call(
        prepare_kernel,
        out_shape=(pltpu.VMEM(inputs.shape, inputs.dtype),) * 2,
        in_specs=[smem] + [hbm] * 5,
        out_specs=[vmem] * 2,
        scratch_shapes=[pltpu.VMEM(v.shape, v.dtype) for v in saved]
        + [pltpu.SemaphoreType.DMA((5,))],
        compiler_params=params,
        name="prepare",
    )(place, *(pltpu.with_memory_space_constraint(v, pltpu.HBM) for v in saved))
    sets = gather_operands(keep, send, fs_size, tp_size)
    model = inputs.shape[1] * tp_size
    total = 2 * query_grad.shape[1] * tp_size
    sides = (
        (query_rows, query_row_root, query_weight, query_moment, query_cols, query_col_root),
        (forget_rows, forget_row_root, forget_weight, forget_moment, forget_cols, forget_col_root),
    )
    wide = jax.ShapeDtypeStruct(query_weight.shape, jnp.float32)
    narrow = jax.ShapeDtypeStruct(query_weight.shape, jnp.bfloat16)
    row_kind = jax.ShapeDtypeStruct(query_rows.shape, jnp.float32)
    col_kind = jax.ShapeDtypeStruct(query_cols.shape, jnp.float32)
    kinds = (wide, narrow, wide, wide, row_kind, col_kind)
    held = []
    for side in sides:
        held += [pltpu.VMEM(v.shape, v.dtype) for v in side]
        held += [pltpu.VMEM(k.shape, k.dtype) for k in kinds[:4]]
    anywhere = pl.BlockSpec(memory_space=pl.ANY)
    set_scratch = [
        pltpu.VMEM((2 * inputs.shape[0], model), jnp.bfloat16),
        pltpu.VMEM((2 * inputs.shape[0], total), jnp.bfloat16),
    ]
    acc = []
    for pieces in sets[:-1]:
        acc = [
            pl.pallas_call(
                partial(sum_kernel, not acc),
                out_shape=pltpu.VMEM((model, total), jnp.float32),
                in_specs=[smem] + [anywhere] * 4 + [vmem] * len(acc),
                out_specs=vmem,
                scratch_shapes=set_scratch + [pltpu.SemaphoreType.DMA((2,))],
                input_output_aliases={5: 0} if acc else {},
                compiler_params=params,
            )(place, *pieces, *acc)
        ]
    operands = [*sets[-1], pltpu.with_memory_space_constraint(*acc, pltpu.VMEM)]
    operands += [pltpu.with_memory_space_constraint(v, pltpu.HBM) for side in sides for v in side]
    out = pl.pallas_call(
        tail_kernel,
        out_shape=kinds * 2,
        in_specs=[smem] + [anywhere] * 4 + [vmem] + [hbm] * 12,
        out_specs=[hbm] * 12,
        scratch_shapes=set_scratch
        + [
            pltpu.VMEM((model, total), jnp.bfloat16),
            pltpu.SemaphoreType.DMA((2,)),
            pltpu.SemaphoreType.DMA((2, 6)),
            pltpu.SemaphoreType.DMA((2, 6)),
        ]
        + held,
        compiler_params=params,
        name="tail",
    )(place, *operands)
    return tuple(v for both in zip(out[:6], out[6:], strict=True) for v in both)


def use_gathered(tokens, model, hidden, fs_size, tp_size):
    blocks = fs_size // 2
    square_grid = tp_size == 4 and fs_size % 2 == 0 and blocks & (blocks - 1) == 0
    return square_grid and tokens * (model + 2 * hidden) <= model * 2 * hidden


def on_device(fs_size, tp_size, inputs, query_grad, forget_grad, forget_pre, lower_bound, *rest):
    tokens = inputs.shape[0] * fs_size
    if use_gathered(tokens, inputs.shape[1] * tp_size, query_grad.shape[1] * tp_size, fs_size, tp_size):
        return gathered_plan(
            inputs, query_grad, forget_grad, forget_pre, lower_bound, *rest, fs_size, tp_size
        )
    sigma_gate = jax.nn.sigmoid(forget_pre.astype(jnp.float32))
    forget_cot = (
        forget_grad.astype(jnp.float32) * (1.0 - lower_bound) * sigma_gate * (1.0 - sigma_gate)
    ).astype(jnp.bfloat16)
    return summed_plan(inputs, query_grad, forget_cot, *rest)


def solution(mesh):
    in_specs = (
        P("fs", "tp"),
        P("fs", "tp"),
        P("fs", "tp"),
        P("fs", "tp"),
        P("tp"),
        P("fs", "tp"),
        P("fs", "tp"),
        P("fs", "tp"),
        P("fs", "tp"),
        P("fs", None),
        P("fs", None),
        P("tp", None, None),
        P("tp", None, None),
        P("fs", None),
        P("fs", None),
        P("tp", None, None),
        P("tp", None, None),
    )
    out_specs = (
        P("fs", "tp"),
        P("fs", "tp"),
        P("fs", "tp"),
        P("fs", "tp"),
        P("fs", "tp"),
        P("fs", "tp"),
        P("fs", "tp"),
        P("fs", "tp"),
        P("fs", None),
        P("fs", None),
        P("tp", None, None),
        P("tp", None, None),
    )
    sizes = (mesh.shape["fs"], mesh.shape["tp"])
    return jax.shard_map(
        partial(on_device, *sizes), mesh=mesh, in_specs=in_specs, out_specs=out_specs, check_vma=False
    )
```

```python
from functools import partial

import jax
import jax.numpy as jnp
from jax import lax
from jax.experimental import pallas as pl
from jax.experimental.pallas import tpu as pltpu
from jax.sharding import PartitionSpec as P


D = 2048
HW = 1024
HEAD = 128


stat_decay = 0.9
moment_decay = 0.9
learn_rate = 0.02
highest = lax.Precision.HIGHEST


def fold_one(carry_state, shard_piece, offset, root_mine, grad_mine):
    left_sum, outer_rows, column_total = carry_state
    row_count, col_width = shard_piece.shape
    left_sum = left_sum + jnp.dot(root_mine, shard_piece, precision=highest)
    outer_piece = lax.dot_general(
        grad_mine, shard_piece, (((1,), (1,)), ((), ())), precision=highest
    )
    outer_rows = lax.dynamic_update_slice_in_dim(outer_rows, outer_piece, offset, 1)
    by_head = shard_piece.reshape(row_count, col_width // HEAD, HEAD)
    column_total = column_total + jnp.einsum("rhi,rhj->hij", by_head, by_head, precision=highest)
    return (left_sum, outer_rows, column_total)


def finish(weight, moment, rows, cols, col_root, left_sum, outer_rows, column_total, square):
    norm_scale = jnp.sqrt(D * HW / (square + 1.0))
    scale_twice = norm_scale * norm_scale
    rows_next = stat_decay * rows + (1.0 - stat_decay) / HW * scale_twice * outer_rows
    cols_next = stat_decay * cols + (1.0 - stat_decay) / D * scale_twice * column_total
    shard_rows, col_width = left_sum.shape
    shaped = left_sum.reshape(shard_rows, col_width // HEAD, HEAD)
    precond = norm_scale * jnp.einsum(
        "rhi,hij->rhj", shaped, col_root.astype(jnp.float32), precision=highest
    ).reshape(shard_rows, col_width)
    moment_next = moment_decay * moment + (1.0 - moment_decay) * precond
    update_step = moment_decay * moment_next + (1.0 - moment_decay) * precond
    master = weight - learn_rate * update_step
    return (master, master.astype(jnp.bfloat16), update_step, moment_next, rows_next, cols_next)


def summed_plan(
    inputs,
    query_grad,
    forget_cot,
    query_weight,
    forget_weight,
    query_moment,
    forget_moment,
    query_rows,
    forget_rows,
    query_cols,
    forget_cols,
    query_row_root,
    forget_row_root,
    query_col_root,
    forget_col_root,
):
    gathered = lax.all_gather(inputs, "tp", axis=1, tiled=True)
    shard_rows, col_width = query_weight.shape
    heads_here = col_width // HEAD
    row_roots = (query_row_root.astype(jnp.float32), forget_row_root.astype(jnp.float32))
    empty = (
        jnp.zeros((shard_rows, col_width), jnp.float32),
        jnp.zeros((shard_rows, D), jnp.float32),
        jnp.zeros((heads_here, HEAD, HEAD), jnp.float32),
    )
    joined = jnp.concatenate([query_grad, forget_cot], axis=1)
    summed = lax.psum_scatter(
        lax.dot_general(
            gathered, joined, (((0,), (0,)), ((), ())), preferred_element_type=jnp.float32
        ),
        "fs",
        scatter_dimension=0,
        tiled=True,
    )
    gradients = (summed[:, :col_width], summed[:, col_width:])
    offset = jnp.int32(0)
    results = (
        fold_one(
            empty,
            lax.all_gather(gradients[0].astype(jnp.bfloat16), "fs", axis=0, tiled=True).astype(
                jnp.float32
            ),
            offset,
            row_roots[0],
            gradients[0],
        ),
        fold_one(
            empty,
            lax.all_gather(gradients[1].astype(jnp.bfloat16), "fs", axis=0, tiled=True).astype(
                jnp.float32
            ),
            offset,
            row_roots[1],
            gradients[1],
        ),
    )
    query_trace = jnp.sum(jnp.diagonal(results[0][2], axis1=1, axis2=2))
    forget_trace = jnp.sum(jnp.diagonal(results[1][2], axis1=1, axis2=2))
    query_outer, forget_outer, query_square, forget_square = (
        lax.psum(results[0][1].astype(jnp.bfloat16), "tp").astype(jnp.float32),
        lax.psum(results[1][1].astype(jnp.bfloat16), "tp").astype(jnp.float32),
        lax.psum(query_trace.astype(jnp.bfloat16), "tp").astype(jnp.float32),
        lax.psum(forget_trace.astype(jnp.bfloat16), "tp").astype(jnp.float32),
    )
    query_out = finish(
        query_weight,
        query_moment,
        query_rows,
        query_cols,
        query_col_root,
        results[0][0],
        query_outer,
        results[0][2],
        query_square,
    )
    forget_out = finish(
        forget_weight,
        forget_moment,
        forget_rows,
        forget_cols,
        forget_col_root,
        results[1][0],
        forget_outer,
        results[1][2],
        forget_square,
    )
    return (
        query_out[0],
        forget_out[0],
        query_out[1],
        forget_out[1],
        query_out[2],
        forget_out[2],
        query_out[3],
        forget_out[3],
        query_out[4],
        forget_out[4],
        query_out[5],
        forget_out[5],
    )


def linear_pairs(fs_size, tp_size, target):
    pairs = []
    for f in range(fs_size):
        for t in range(tp_size):
            to_f, to_t = target(f, t)
            pairs.append((f * tp_size + t, to_f * tp_size + to_t))
    return pairs


def gather_operands(keep, send, fs_size, tp_size):
    axes = ("fs", "tp")

    def move(value, target):
        return lax.ppermute(value, axes, linear_pairs(fs_size, tp_size, target))

    def partner(f, t):
        return (f, t ^ 1)

    def first_hop(f, t):
        return (f ^ 1, t) if t % 2 == 0 else (f, t ^ 2)

    def second_hop(f, t):
        return (f, t ^ 2) if t % 2 == 0 else (f ^ 1, t)

    lanes = [jnp.stack([keep, move(send, partner)])]
    for k in range(1, fs_size // 2):
        step = k & -k if k & (k - 1) == 0 else k & (k - 1) ^ k
        source = lanes[k ^ step]
        lanes.append(move(source, lambda f, t, step=step: (f ^ (2 * step), t)))
    sets = []
    nears = []
    for s, lane in enumerate(lanes):
        if s & 1:
            nears.append(move(nears[s ^ 1], lambda f, t: (f ^ 2, t)))
        else:
            nears.append(move(lane, first_hop))
        pair = jnp.stack([lane, nears[s]])
        far = move(pair, second_hop)
        sets.append((pair, far, move(pair, partner), move(far, partner)))
    return sets


def assemble(place, pieces, x_set, y_set, sem):
    odd, upper = place[0], place[1]
    tokens, width = pieces[0].shape[2:]
    own = width // 2
    hidden = y_set.shape[1] // 2

    def copies(x_pieces, y_pieces):
        for p in range(2):
            rows = pl.ds(p * tokens, tokens)
            for h in range(2):
                for c in range(2):
                    col = pl.multiple_of(((upper ^ h) * 2 + c) * width, width)
                    pltpu.make_async_copy(
                        x_pieces[h].at[p, c], x_set.at[rows, pl.ds(col, width)], sem.at[0]
                    ).start()
                    for i in range(2):
                        pltpu.make_async_copy(
                            y_pieces[p].at[h, 1 - c, :, pl.ds(i * own, own)],
                            y_set.at[rows, pl.ds(i * hidden + (2 * h + c) * own, own)],
                            sem.at[1],
                        ).start()

    pair, far, pair_other, far_other = pieces

    @pl.when(odd == 0)
    def _():
        copies((pair, far), (pair_other, far_other))

    @pl.when(odd == 1)
    def _():
        copies((pair_other, far_other), (pair, far))


def assembled(x_set, y_set, sem):
    for k, whole in enumerate((x_set, y_set)):
        pltpu.make_async_copy(whole, whole, sem.at[k]).wait()


def product(x_set, y_set, cols):
    return lax.dot_general(
        x_set[...], y_set[:, cols], (((0,), (0,)), ((), ())), preferred_element_type=jnp.float32
    )


def sum_kernel(first, place, *refs):
    pieces, refs = refs[:4], refs[4:]
    if not first:
        refs = refs[1:]
    acc, x_set, y_set, sem = refs
    assemble(place, pieces, x_set, y_set, sem)
    assembled(x_set, y_set, sem)
    total, chunk = acc.shape[1], x_set.shape[0]
    for at in range(0, total, chunk):
        cols = slice(at, at + chunk)
        part = product(x_set, y_set, cols)
        acc[:, cols] = part if first else acc[:, cols] + part


def tail_kernel(place, *refs):
    pieces, acc, refs = refs[:4], refs[4], refs[5:]
    sides = [refs[6 * i : 6 * i + 6] for i in range(2)]
    refs = refs[12:]
    outs = [refs[6 * i : 6 * i + 6] for i in range(2)]
    refs = refs[12:]
    x_set, y_set, grad, sem, load_sem, store_sem = refs[:6]
    held = [refs[6 + 10 * i : 16 + 10 * i] for i in range(2)]
    odd, band = place[0], place[2]
    model, total = grad.shape
    hidden = total // 2
    own = pieces[0].shape[3] // 2
    rows_here = held[0][0].shape[0]

    assemble(place, pieces, x_set, y_set, sem)
    loads = [
        [
            pltpu.make_async_copy(src, dst, load_sem.at[i, j])
            for j, (src, dst) in enumerate(zip(sides[i], held[i][:6], strict=True))
        ]
        for i in range(2)
    ]
    for side in loads:
        for copy in side:
            copy.start()
    assembled(x_set, y_set, sem)

    chunk = x_set.shape[0]
    squares = [jnp.zeros((8, chunk), jnp.float32)] * 2
    for at in range(0, total, chunk):
        cols = slice(at, at + chunk)
        part = acc[:, cols] + product(x_set, y_set, cols)
        grad[:, cols] = part.astype(jnp.bfloat16)
        squares[at // hidden] += jnp.sum((part * part).reshape(-1, 8, chunk), axis=0)

    stores = []
    first = pl.multiple_of(band * rows_here, rows_here)
    for i in range(2):
        rows, row_root, weight, moment, cols, col_root = held[i][:6]
        master_out, copy_out, step_out, moment_out = held[i][6:]
        for copy in loads[i]:
            copy.wait()
        square = jnp.sum(squares[i], keepdims=True)
        scale = jnp.sqrt(model * hidden / (square + 1.0))
        twice = scale * scale
        mine = pl.multiple_of(i * hidden + odd * own, own)
        band_grad = grad[pl.ds(first, rows_here), i * hidden : (i + 1) * hidden]
        row_factor = (1.0 - stat_decay) / hidden * twice

        for at in range(0, model, own * 2):
            part = lax.dot_general(
                band_grad,
                grad[at : at + own * 2, i * hidden : (i + 1) * hidden],
                (((1,), (1,)), ((), ())),
                preferred_element_type=jnp.float32,
            )
            to = slice(at, at + own * 2)
            rows[:, to] = stat_decay * rows[:, to] + row_factor * part
        stores.append(pltpu.make_async_copy(rows, outs[i][4], store_sem.at[i, 4]))
        stores[-1].start()
        own_grad = grad[:, pl.ds(mine, own)]
        column_total = lax.dot_general(
            own_grad, own_grad, (((0,), (0,)), ((), ())), preferred_element_type=jnp.float32
        )
        left = jnp.dot(row_root[...], own_grad, preferred_element_type=jnp.float32)
        left_high = left.astype(jnp.bfloat16)
        left_low = (left - left_high.astype(jnp.float32)).astype(jnp.bfloat16)
        for h in range(own // HEAD):
            at = slice(h * HEAD, (h + 1) * HEAD)
            cols[h] = (
                stat_decay * cols[h]
                + (1.0 - stat_decay) / model * twice * column_total[at, at]
            )
            root = col_root[h]
            precond = scale * (
                jnp.dot(left_high[:, at], root, preferred_element_type=jnp.float32)
                + jnp.dot(left_low[:, at], root, preferred_element_type=jnp.float32)
            )
            moment_next = moment_decay * moment[:, at] + (1.0 - moment_decay) * precond
            update_step = moment_decay * moment_next + (1.0 - moment_decay) * precond
            master = weight[:, at] - learn_rate * update_step
            master_out[:, at] = master
            copy_out[:, at] = master.astype(jnp.bfloat16)
            step_out[:, at] = update_step
            moment_out[:, at] = moment_next
        for src, dst in ((master_out, 0), (copy_out, 1), (step_out, 2), (moment_out, 3), (cols, 5)):
            stores.append(pltpu.make_async_copy(src, outs[i][dst], store_sem.at[i, dst]))
            stores[-1].start()
    for copy in stores:
        copy.wait()


def prepare_kernel(place, *refs):
    sources, (keep, send), held, sem = refs[:5], refs[5:7], refs[7:12], refs[12]
    copies = [
        pltpu.make_async_copy(src, dst, sem.at[j])
        for j, (src, dst) in enumerate(zip(sources, held, strict=True))
    ]
    for copy in copies:
        copy.start()
    for copy in copies:
        copy.wait()
    inputs, query_grad, forget_grad, forget_pre, lower_bound = held
    own = query_grad.shape[1]
    sigma_gate = jax.nn.sigmoid(forget_pre[...].astype(jnp.float32))
    forget_cot = (
        forget_grad[...].astype(jnp.float32)
        * (1.0 - lower_bound[...])
        * sigma_gate
        * (1.0 - sigma_gate)
    ).astype(jnp.bfloat16)

    def write(x_to, y_to):
        x_to[...] = inputs[...]
        y_to[:, :own] = query_grad[...]
        y_to[:, own:] = forget_cot

    @pl.when(place[0] == 0)
    def _():
        write(keep, send)

    @pl.when(place[0] == 1)
    def _():
        write(send, keep)


def gathered_plan(
    inputs,
    query_grad,
    forget_grad,
    forget_pre,
    lower_bound,
    query_weight,
    forget_weight,
    query_moment,
    forget_moment,
    query_rows,
    forget_rows,
    query_cols,
    forget_cols,
    query_row_root,
    forget_row_root,
    query_col_root,
    forget_col_root,
    fs_size,
    tp_size,
):
    tp_at = lax.axis_index("tp")
    place = jnp.stack([tp_at & 1, tp_at >> 1, lax.axis_index("fs")]).astype(jnp.int32)
    smem = pl.BlockSpec(memory_space=pltpu.SMEM)
    vmem = pl.BlockSpec(memory_space=pltpu.VMEM)
    params = pltpu.CompilerParams(vmem_limit_bytes=26 * 2**20)
    hbm = pl.BlockSpec(memory_space=pltpu.HBM)
    saved = (inputs, query_grad, forget_grad, forget_pre, lower_bound[None])
    keep, send = pl.pallas_call(
        prepare_kernel,
        out_shape=(pltpu.VMEM(inputs.shape, inputs.dtype),) * 2,
        in_specs=[smem] + [hbm] * 5,
        out_specs=[vmem] * 2,
        scratch_shapes=[pltpu.VMEM(v.shape, v.dtype) for v in saved]
        + [pltpu.SemaphoreType.DMA((5,))],
        compiler_params=params,
        name="prepare",
    )(place, *(pltpu.with_memory_space_constraint(v, pltpu.HBM) for v in saved))
    sets = gather_operands(keep, send, fs_size, tp_size)
    model = inputs.shape[1] * tp_size
    total = 2 * query_grad.shape[1] * tp_size
    sides = (
        (query_rows, query_row_root, query_weight, query_moment, query_cols, query_col_root),
        (forget_rows, forget_row_root, forget_weight, forget_moment, forget_cols, forget_col_root),
    )
    wide = jax.ShapeDtypeStruct(query_weight.shape, jnp.float32)
    narrow = jax.ShapeDtypeStruct(query_weight.shape, jnp.bfloat16)
    row_kind = jax.ShapeDtypeStruct(query_rows.shape, jnp.float32)
    col_kind = jax.ShapeDtypeStruct(query_cols.shape, jnp.float32)
    kinds = (wide, narrow, wide, wide, row_kind, col_kind)
    held = []
    for side in sides:
        held += [pltpu.VMEM(v.shape, v.dtype) for v in side]
        held += [pltpu.VMEM(k.shape, k.dtype) for k in kinds[:4]]
    anywhere = pl.BlockSpec(memory_space=pl.ANY)
    set_scratch = [
        pltpu.VMEM((2 * inputs.shape[0], model), jnp.bfloat16),
        pltpu.VMEM((2 * inputs.shape[0], total), jnp.bfloat16),
    ]
    acc = []
    for pieces in sets[:-1]:
        acc = [
            pl.pallas_call(
                partial(sum_kernel, not acc),
                out_shape=pltpu.VMEM((model, total), jnp.float32),
                in_specs=[smem] + [anywhere] * 4 + [vmem] * len(acc),
                out_specs=vmem,
                scratch_shapes=set_scratch + [pltpu.SemaphoreType.DMA((2,))],
                input_output_aliases={5: 0} if acc else {},
                compiler_params=params,
            )(place, *pieces, *acc)
        ]
    operands = [*sets[-1], pltpu.with_memory_space_constraint(*acc, pltpu.VMEM)]
    operands += [pltpu.with_memory_space_constraint(v, pltpu.HBM) for side in sides for v in side]
    out = pl.pallas_call(
        tail_kernel,
        out_shape=kinds * 2,
        in_specs=[smem] + [anywhere] * 4 + [vmem] + [hbm] * 12,
        out_specs=[hbm] * 12,
        scratch_shapes=set_scratch
        + [
            pltpu.VMEM((model, total), jnp.bfloat16),
            pltpu.SemaphoreType.DMA((2,)),
            pltpu.SemaphoreType.DMA((2, 6)),
            pltpu.SemaphoreType.DMA((2, 6)),
        ]
        + held,
        compiler_params=params,
        name="tail",
    )(place, *operands)
    return tuple(v for both in zip(out[:6], out[6:], strict=True) for v in both)


def use_gathered(tokens, model, hidden, fs_size, tp_size):
    blocks = fs_size // 2
    square_grid = tp_size == 4 and fs_size % 2 == 0 and blocks & (blocks - 1) == 0
    return square_grid and tokens * (model + 2 * hidden) <= model * 2 * hidden


def on_device(fs_size, tp_size, inputs, query_grad, forget_grad, forget_pre, lower_bound, *rest):
    tokens = inputs.shape[0] * fs_size
    if use_gathered(tokens, inputs.shape[1] * tp_size, query_grad.shape[1] * tp_size, fs_size, tp_size):
        return gathered_plan(
            inputs, query_grad, forget_grad, forget_pre, lower_bound, *rest, fs_size, tp_size
        )
    sigma_gate = jax.nn.sigmoid(forget_pre.astype(jnp.float32))
    forget_cot = (
        forget_grad.astype(jnp.float32) * (1.0 - lower_bound) * sigma_gate * (1.0 - sigma_gate)
    ).astype(jnp.bfloat16)
    return summed_plan(inputs, query_grad, forget_cot, *rest)


def solution(mesh):
    in_specs = (
        P("fs", "tp"),
        P("fs", "tp"),
        P("fs", "tp"),
        P("fs", "tp"),
        P("tp"),
        P("fs", "tp"),
        P("fs", "tp"),
        P("fs", "tp"),
        P("fs", "tp"),
        P("fs", None),
        P("fs", None),
        P("tp", None, None),
        P("tp", None, None),
        P("fs", None),
        P("fs", None),
        P("tp", None, None),
        P("tp", None, None),
    )
    out_specs = (
        P("fs", "tp"),
        P("fs", "tp"),
        P("fs", "tp"),
        P("fs", "tp"),
        P("fs", "tp"),
        P("fs", "tp"),
        P("fs", "tp"),
        P("fs", "tp"),
        P("fs", None),
        P("fs", None),
        P("tp", None, None),
        P("tp", None, None),
    )
    sizes = (mesh.shape["fs"], mesh.shape["tp"])
    return jax.shard_map(
        partial(on_device, *sizes), mesh=mesh, in_specs=in_specs, out_specs=out_specs, check_vma=False
    )
```

```python
from functools import partial

import jax
import jax.numpy as jnp
from jax import lax
from jax.experimental import pallas as pl
from jax.experimental.pallas import tpu as pltpu
from jax.sharding import PartitionSpec as P


D = 2048
HW = 1024
HEAD = 128


stat_decay = 0.9
moment_decay = 0.9
learn_rate = 0.02
highest = lax.Precision.HIGHEST


def fold_one(carry_state, shard_piece, offset, root_mine, grad_mine):
    left_sum, outer_rows, column_total = carry_state
    row_count, col_width = shard_piece.shape
    left_sum = left_sum + jnp.dot(root_mine, shard_piece, precision=highest)
    outer_piece = lax.dot_general(
        grad_mine, shard_piece, (((1,), (1,)), ((), ())), precision=highest
    )
    outer_rows = lax.dynamic_update_slice_in_dim(outer_rows, outer_piece, offset, 1)
    by_head = shard_piece.reshape(row_count, col_width // HEAD, HEAD)
    column_total = column_total + jnp.einsum("rhi,rhj->hij", by_head, by_head, precision=highest)
    return (left_sum, outer_rows, column_total)


def finish(weight, moment, rows, cols, col_root, left_sum, outer_rows, column_total, square):
    norm_scale = jnp.sqrt(D * HW / (square + 1.0))
    scale_twice = norm_scale * norm_scale
    rows_next = stat_decay * rows + (1.0 - stat_decay) / HW * scale_twice * outer_rows
    cols_next = stat_decay * cols + (1.0 - stat_decay) / D * scale_twice * column_total
    shard_rows, col_width = left_sum.shape
    shaped = left_sum.reshape(shard_rows, col_width // HEAD, HEAD)
    precond = norm_scale * jnp.einsum(
        "rhi,hij->rhj", shaped, col_root.astype(jnp.float32), precision=highest
    ).reshape(shard_rows, col_width)
    moment_next = moment_decay * moment + (1.0 - moment_decay) * precond
    update_step = moment_decay * moment_next + (1.0 - moment_decay) * precond
    master = weight - learn_rate * update_step
    return (master, master.astype(jnp.bfloat16), update_step, moment_next, rows_next, cols_next)


def summed_plan(
    inputs,
    query_grad,
    forget_cot,
    query_weight,
    forget_weight,
    query_moment,
    forget_moment,
    query_rows,
    forget_rows,
    query_cols,
    forget_cols,
    query_row_root,
    forget_row_root,
    query_col_root,
    forget_col_root,
):
    gathered = lax.all_gather(inputs, "tp", axis=1, tiled=True)
    shard_rows, col_width = query_weight.shape
    heads_here = col_width // HEAD
    row_roots = (query_row_root.astype(jnp.float32), forget_row_root.astype(jnp.float32))
    empty = (
        jnp.zeros((shard_rows, col_width), jnp.float32),
        jnp.zeros((shard_rows, D), jnp.float32),
        jnp.zeros((heads_here, HEAD, HEAD), jnp.float32),
    )
    joined = jnp.concatenate([query_grad, forget_cot], axis=1)
    summed = lax.psum_scatter(
        lax.dot_general(
            gathered, joined, (((0,), (0,)), ((), ())), preferred_element_type=jnp.float32
        ),
        "fs",
        scatter_dimension=0,
        tiled=True,
    )
    gradients = (summed[:, :col_width], summed[:, col_width:])
    offset = jnp.int32(0)
    results = (
        fold_one(
            empty,
            lax.all_gather(gradients[0].astype(jnp.bfloat16), "fs", axis=0, tiled=True).astype(
                jnp.float32
            ),
            offset,
            row_roots[0],
            gradients[0],
        ),
        fold_one(
            empty,
            lax.all_gather(gradients[1].astype(jnp.bfloat16), "fs", axis=0, tiled=True).astype(
                jnp.float32
            ),
            offset,
            row_roots[1],
            gradients[1],
        ),
    )
    query_trace = jnp.sum(jnp.diagonal(results[0][2], axis1=1, axis2=2))
    forget_trace = jnp.sum(jnp.diagonal(results[1][2], axis1=1, axis2=2))
    query_outer, forget_outer, query_square, forget_square = (
        lax.psum(results[0][1].astype(jnp.bfloat16), "tp").astype(jnp.float32),
        lax.psum(results[1][1].astype(jnp.bfloat16), "tp").astype(jnp.float32),
        lax.psum(query_trace.astype(jnp.bfloat16), "tp").astype(jnp.float32),
        lax.psum(forget_trace.astype(jnp.bfloat16), "tp").astype(jnp.float32),
    )
    query_out = finish(
        query_weight,
        query_moment,
        query_rows,
        query_cols,
        query_col_root,
        results[0][0],
        query_outer,
        results[0][2],
        query_square,
    )
    forget_out = finish(
        forget_weight,
        forget_moment,
        forget_rows,
        forget_cols,
        forget_col_root,
        results[1][0],
        forget_outer,
        results[1][2],
        forget_square,
    )
    return (
        query_out[0],
        forget_out[0],
        query_out[1],
        forget_out[1],
        query_out[2],
        forget_out[2],
        query_out[3],
        forget_out[3],
        query_out[4],
        forget_out[4],
        query_out[5],
        forget_out[5],
    )


def linear_pairs(fs_size, tp_size, target):
    pairs = []
    for f in range(fs_size):
        for t in range(tp_size):
            to_f, to_t = target(f, t)
            pairs.append((f * tp_size + t, to_f * tp_size + to_t))
    return pairs


def gather_operands(keep, send, fs_size, tp_size):
    axes = ("fs", "tp")

    def move(value, target):
        return lax.ppermute(value, axes, linear_pairs(fs_size, tp_size, target))

    def partner(f, t):
        return (f, t ^ 1)

    def first_hop(f, t):
        return (f ^ 1, t) if t % 2 == 0 else (f, t ^ 2)

    def second_hop(f, t):
        return (f, t ^ 2) if t % 2 == 0 else (f ^ 1, t)

    lanes = [jnp.stack([keep, move(send, partner)])]
    for k in range(1, fs_size // 2):
        step = k & -k if k & (k - 1) == 0 else k & (k - 1) ^ k
        source = lanes[k ^ step]
        lanes.append(move(source, lambda f, t, step=step: (f ^ (2 * step), t)))
    sets = []
    nears = []
    for s, lane in enumerate(lanes):
        if s & 1:
            nears.append(move(nears[s ^ 1], lambda f, t: (f ^ 2, t)))
        else:
            nears.append(move(lane, first_hop))
        pair = jnp.stack([lane, nears[s]])
        far = move(pair, second_hop)
        sets.append((pair, far, move(pair, partner), move(far, partner)))
    return sets


def assemble(place, pieces, x_set, y_set, sem):
    odd, upper = place[0], place[1]
    tokens, width = pieces[0].shape[2:]
    own = width // 2
    hidden = y_set.shape[1] // 2

    def copies(x_pieces, y_pieces):
        for p in range(2):
            rows = pl.ds(p * tokens, tokens)
            for h in range(2):
                for c in range(2):
                    col = pl.multiple_of(((upper ^ h) * 2 + c) * width, width)
                    pltpu.make_async_copy(
                        x_pieces[h].at[p, c], x_set.at[rows, pl.ds(col, width)], sem.at[0]
                    ).start()
                    for i in range(2):
                        pltpu.make_async_copy(
                            y_pieces[p].at[h, 1 - c, :, pl.ds(i * own, own)],
                            y_set.at[rows, pl.ds(i * hidden + (2 * h + c) * own, own)],
                            sem.at[1],
                        ).start()

    pair, far, pair_other, far_other = pieces

    @pl.when(odd == 0)
    def _():
        copies((pair, far), (pair_other, far_other))

    @pl.when(odd == 1)
    def _():
        copies((pair_other, far_other), (pair, far))


def assembled(x_set, y_set, sem):
    for k, whole in enumerate((x_set, y_set)):
        pltpu.make_async_copy(whole, whole, sem.at[k]).wait()


def product(x_set, y_set, cols):
    return lax.dot_general(
        x_set[...], y_set[:, cols], (((0,), (0,)), ((), ())), preferred_element_type=jnp.float32
    )


def sum_kernel(first, place, *refs):
    pieces, refs = refs[:4], refs[4:]
    if not first:
        refs = refs[1:]
    acc, x_set, y_set, sem = refs
    assemble(place, pieces, x_set, y_set, sem)
    assembled(x_set, y_set, sem)
    total, chunk = acc.shape[1], x_set.shape[0]
    for at in range(0, total, chunk):
        cols = slice(at, at + chunk)
        part = product(x_set, y_set, cols)
        acc[:, cols] = part if first else acc[:, cols] + part


def tail_kernel(place, *refs):
    pieces, acc, refs = refs[:4], refs[4], refs[5:]
    sides = [refs[6 * i : 6 * i + 6] for i in range(2)]
    refs = refs[12:]
    outs = [refs[6 * i : 6 * i + 6] for i in range(2)]
    refs = refs[12:]
    x_set, y_set, grad, sem, load_sem, store_sem = refs[:6]
    held = [refs[6 + 10 * i : 16 + 10 * i] for i in range(2)]
    odd, band = place[0], place[2]
    model, total = grad.shape
    hidden = total // 2
    own = pieces[0].shape[3] // 2
    rows_here = held[0][0].shape[0]

    assemble(place, pieces, x_set, y_set, sem)
    loads = [
        [
            pltpu.make_async_copy(src, dst, load_sem.at[i, j])
            for j, (src, dst) in enumerate(zip(sides[i], held[i][:6], strict=True))
        ]
        for i in range(2)
    ]
    assembled(x_set, y_set, sem)
    for j in (1, 2, 3, 4, 5, 0):
        for side in loads:
            side[j].start()

    chunk = x_set.shape[0]
    squares = [jnp.zeros((8, chunk), jnp.float32)] * 2
    for at in range(0, total, chunk):
        cols = slice(at, at + chunk)
        part = acc[:, cols] + product(x_set, y_set, cols)
        grad[:, cols] = part.astype(jnp.bfloat16)
        squares[at // hidden] += jnp.sum((part * part).reshape(-1, 8, chunk), axis=0)

    stores = []

    def store(src, dst, at):
        stores.append(pltpu.make_async_copy(src, dst, store_sem.at[at]))
        stores[-1].start()

    scales = []
    for i in range(2):
        _, row_root, weight, moment, cols, col_root = held[i][:6]
        results = held[i][6:]
        square = jnp.sum(squares[i], keepdims=True)
        scale = jnp.sqrt(model * hidden / (square + 1.0))
        scales.append(scale)
        mine = pl.multiple_of(i * hidden + odd * own, own)
        own_grad = grad[:, pl.ds(mine, own)]
        loads[i][1].wait()
        left = jnp.dot(row_root[...], own_grad, preferred_element_type=jnp.float32)
        left_high = left.astype(jnp.bfloat16)
        left_low = (left - left_high.astype(jnp.float32)).astype(jnp.bfloat16)
        column_total = lax.dot_general(
            own_grad, own_grad, (((0,), (0,)), ((), ())), preferred_element_type=jnp.float32
        )
        for copy in loads[i][2:]:
            copy.wait()
        for h in range(own // HEAD):
            at = slice(h * HEAD, (h + 1) * HEAD)
            cols[h] = (
                stat_decay * cols[h]
                + (1.0 - stat_decay) / model * scale * scale * column_total[at, at]
            )
            root = col_root[h]
            precond = scale * (
                jnp.dot(left_high[:, at], root, preferred_element_type=jnp.float32)
                + jnp.dot(left_low[:, at], root, preferred_element_type=jnp.float32)
            )
            moment_next = moment_decay * moment[:, at] + (1.0 - moment_decay) * precond
            update_step = moment_decay * moment_next + (1.0 - moment_decay) * precond
            master = weight[:, at] - learn_rate * update_step
            for to, value in zip(
                results,
                (master, master.astype(jnp.bfloat16), update_step, moment_next),
                strict=True,
            ):
                to[:, at] = value
        for j, src in enumerate(results):
            store(src, outs[i][j], (i, j))
        store(cols, outs[i][5], (i, 4))
    first = pl.multiple_of(band * rows_here, rows_here)
    piece = 2 * own
    for i in range(2):
        rows = held[i][0]
        loads[i][0].wait()
        band_grad = grad[pl.ds(first, rows_here), i * hidden : (i + 1) * hidden]
        factor = (1.0 - stat_decay) / hidden * scales[i] * scales[i]
        for k in range(model // piece):
            at = slice(k * piece, (k + 1) * piece)
            part = lax.dot_general(
                band_grad,
                grad[at, i * hidden : (i + 1) * hidden],
                (((1,), (1,)), ((), ())),
                preferred_element_type=jnp.float32,
            )
            rows[:, at] = stat_decay * rows[:, at] + factor * part
            store(rows.at[:, at], outs[i][4].at[:, at], (i, 5 + k))
    for copy in stores:
        copy.wait()


def prepare_kernel(place, *refs):
    sources, (keep, send), held, sem = refs[:5], refs[5:7], refs[7:12], refs[12]
    copies = [
        pltpu.make_async_copy(src, dst, sem.at[j])
        for j, (src, dst) in enumerate(zip(sources, held, strict=True))
    ]
    for copy in copies:
        copy.start()
    for copy in copies:
        copy.wait()
    inputs, query_grad, forget_grad, forget_pre, lower_bound = held
    own = query_grad.shape[1]
    sigma_gate = jax.nn.sigmoid(forget_pre[...].astype(jnp.float32))
    forget_cot = (
        forget_grad[...].astype(jnp.float32)
        * (1.0 - lower_bound[...])
        * sigma_gate
        * (1.0 - sigma_gate)
    ).astype(jnp.bfloat16)

    def write(x_to, y_to):
        x_to[...] = inputs[...]
        y_to[:, :own] = query_grad[...]
        y_to[:, own:] = forget_cot

    @pl.when(place[0] == 0)
    def _():
        write(keep, send)

    @pl.when(place[0] == 1)
    def _():
        write(send, keep)


def gathered_plan(
    inputs,
    query_grad,
    forget_grad,
    forget_pre,
    lower_bound,
    query_weight,
    forget_weight,
    query_moment,
    forget_moment,
    query_rows,
    forget_rows,
    query_cols,
    forget_cols,
    query_row_root,
    forget_row_root,
    query_col_root,
    forget_col_root,
    fs_size,
    tp_size,
):
    tp_at = lax.axis_index("tp")
    place = jnp.stack([tp_at & 1, tp_at >> 1, lax.axis_index("fs")]).astype(jnp.int32)
    smem = pl.BlockSpec(memory_space=pltpu.SMEM)
    vmem = pl.BlockSpec(memory_space=pltpu.VMEM)
    params = pltpu.CompilerParams(vmem_limit_bytes=26 * 2**20)
    hbm = pl.BlockSpec(memory_space=pltpu.HBM)
    saved = (inputs, query_grad, forget_grad, forget_pre, lower_bound[None])
    keep, send = pl.pallas_call(
        prepare_kernel,
        out_shape=(pltpu.VMEM(inputs.shape, inputs.dtype),) * 2,
        in_specs=[smem] + [hbm] * 5,
        out_specs=[vmem] * 2,
        scratch_shapes=[pltpu.VMEM(v.shape, v.dtype) for v in saved]
        + [pltpu.SemaphoreType.DMA((5,))],
        compiler_params=params,
        name="prepare",
    )(place, *(pltpu.with_memory_space_constraint(v, pltpu.HBM) for v in saved))
    sets = gather_operands(keep, send, fs_size, tp_size)
    model = inputs.shape[1] * tp_size
    total = 2 * query_grad.shape[1] * tp_size
    sides = (
        (query_rows, query_row_root, query_weight, query_moment, query_cols, query_col_root),
        (forget_rows, forget_row_root, forget_weight, forget_moment, forget_cols, forget_col_root),
    )
    wide = jax.ShapeDtypeStruct(query_weight.shape, jnp.float32)
    narrow = jax.ShapeDtypeStruct(query_weight.shape, jnp.bfloat16)
    row_kind = jax.ShapeDtypeStruct(query_rows.shape, jnp.float32)
    col_kind = jax.ShapeDtypeStruct(query_cols.shape, jnp.float32)
    kinds = (wide, narrow, wide, wide, row_kind, col_kind)
    held = []
    for side in sides:
        held += [pltpu.VMEM(v.shape, v.dtype) for v in side]
        held += [pltpu.VMEM(k.shape, k.dtype) for k in kinds[:4]]
    anywhere = pl.BlockSpec(memory_space=pl.ANY)
    set_scratch = [
        pltpu.VMEM((2 * inputs.shape[0], model), jnp.bfloat16),
        pltpu.VMEM((2 * inputs.shape[0], total), jnp.bfloat16),
    ]
    acc = []
    for pieces in sets[:-1]:
        acc = [
            pl.pallas_call(
                partial(sum_kernel, not acc),
                out_shape=pltpu.VMEM((model, total), jnp.float32),
                in_specs=[smem] + [anywhere] * 4 + [vmem] * len(acc),
                out_specs=vmem,
                scratch_shapes=set_scratch + [pltpu.SemaphoreType.DMA((2,))],
                input_output_aliases={5: 0} if acc else {},
                compiler_params=params,
            )(place, *pieces, *acc)
        ]
    operands = [*sets[-1], pltpu.with_memory_space_constraint(*acc, pltpu.VMEM)]
    operands += [pltpu.with_memory_space_constraint(v, pltpu.HBM) for side in sides for v in side]
    out = pl.pallas_call(
        tail_kernel,
        out_shape=kinds * 2,
        in_specs=[smem] + [anywhere] * 4 + [vmem] + [hbm] * 12,
        out_specs=[hbm] * 12,
        scratch_shapes=set_scratch
        + [
            pltpu.VMEM((model, total), jnp.bfloat16),
            pltpu.SemaphoreType.DMA((2,)),
            pltpu.SemaphoreType.DMA((2, 6)),
            pltpu.SemaphoreType.DMA((2, 5 + model // query_weight.shape[1] // 2)),
        ]
        + held,
        compiler_params=params,
        name="tail",
    )(place, *operands)
    return tuple(v for both in zip(out[:6], out[6:], strict=True) for v in both)


def use_gathered(tokens, model, hidden, fs_size, tp_size):
    blocks = fs_size // 2
    square_grid = tp_size == 4 and fs_size % 2 == 0 and blocks & (blocks - 1) == 0
    return square_grid and tokens * (model + 2 * hidden) <= model * 2 * hidden


def on_device(fs_size, tp_size, inputs, query_grad, forget_grad, forget_pre, lower_bound, *rest):
    tokens = inputs.shape[0] * fs_size
    if use_gathered(tokens, inputs.shape[1] * tp_size, query_grad.shape[1] * tp_size, fs_size, tp_size):
        return gathered_plan(
            inputs, query_grad, forget_grad, forget_pre, lower_bound, *rest, fs_size, tp_size
        )
    sigma_gate = jax.nn.sigmoid(forget_pre.astype(jnp.float32))
    forget_cot = (
        forget_grad.astype(jnp.float32) * (1.0 - lower_bound) * sigma_gate * (1.0 - sigma_gate)
    ).astype(jnp.bfloat16)
    return summed_plan(inputs, query_grad, forget_cot, *rest)


def solution(mesh):
    in_specs = (
        P("fs", "tp"),
        P("fs", "tp"),
        P("fs", "tp"),
        P("fs", "tp"),
        P("tp"),
        P("fs", "tp"),
        P("fs", "tp"),
        P("fs", "tp"),
        P("fs", "tp"),
        P("fs", None),
        P("fs", None),
        P("tp", None, None),
        P("tp", None, None),
        P("fs", None),
        P("fs", None),
        P("tp", None, None),
        P("tp", None, None),
    )
    out_specs = (
        P("fs", "tp"),
        P("fs", "tp"),
        P("fs", "tp"),
        P("fs", "tp"),
        P("fs", "tp"),
        P("fs", "tp"),
        P("fs", "tp"),
        P("fs", "tp"),
        P("fs", None),
        P("fs", None),
        P("tp", None, None),
        P("tp", None, None),
    )
    sizes = (mesh.shape["fs"], mesh.shape["tp"])
    return jax.shard_map(
        partial(on_device, *sizes), mesh=mesh, in_specs=in_specs, out_specs=out_specs, check_vma=False
    )
```

```python
from functools import partial

import jax
import jax.numpy as jnp
from jax import lax
from jax.experimental import pallas as pl
from jax.experimental.pallas import tpu as pltpu
from jax.sharding import PartitionSpec as P


D = 2048
HW = 1024
HEAD = 128


stat_decay = 0.9
moment_decay = 0.9
learn_rate = 0.02
highest = lax.Precision.HIGHEST


def fold_one(carry_state, shard_piece, offset, root_mine, grad_mine):
    left_sum, outer_rows, column_total = carry_state
    row_count, col_width = shard_piece.shape
    left_sum = left_sum + jnp.dot(root_mine, shard_piece, precision=highest)
    outer_piece = lax.dot_general(
        grad_mine, shard_piece, (((1,), (1,)), ((), ())), precision=highest
    )
    outer_rows = lax.dynamic_update_slice_in_dim(outer_rows, outer_piece, offset, 1)
    by_head = shard_piece.reshape(row_count, col_width // HEAD, HEAD)
    column_total = column_total + jnp.einsum("rhi,rhj->hij", by_head, by_head, precision=highest)
    return (left_sum, outer_rows, column_total)


def finish(weight, moment, rows, cols, col_root, left_sum, outer_rows, column_total, square):
    norm_scale = jnp.sqrt(D * HW / (square + 1.0))
    scale_twice = norm_scale * norm_scale
    rows_next = stat_decay * rows + (1.0 - stat_decay) / HW * scale_twice * outer_rows
    cols_next = stat_decay * cols + (1.0 - stat_decay) / D * scale_twice * column_total
    shard_rows, col_width = left_sum.shape
    shaped = left_sum.reshape(shard_rows, col_width // HEAD, HEAD)
    precond = norm_scale * jnp.einsum(
        "rhi,hij->rhj", shaped, col_root.astype(jnp.float32), precision=highest
    ).reshape(shard_rows, col_width)
    moment_next = moment_decay * moment + (1.0 - moment_decay) * precond
    update_step = moment_decay * moment_next + (1.0 - moment_decay) * precond
    master = weight - learn_rate * update_step
    return (master, master.astype(jnp.bfloat16), update_step, moment_next, rows_next, cols_next)


def summed_plan(
    inputs,
    query_grad,
    forget_cot,
    query_weight,
    forget_weight,
    query_moment,
    forget_moment,
    query_rows,
    forget_rows,
    query_cols,
    forget_cols,
    query_row_root,
    forget_row_root,
    query_col_root,
    forget_col_root,
):
    gathered = lax.all_gather(inputs, "tp", axis=1, tiled=True)
    shard_rows, col_width = query_weight.shape
    heads_here = col_width // HEAD
    row_roots = (query_row_root.astype(jnp.float32), forget_row_root.astype(jnp.float32))
    empty = (
        jnp.zeros((shard_rows, col_width), jnp.float32),
        jnp.zeros((shard_rows, D), jnp.float32),
        jnp.zeros((heads_here, HEAD, HEAD), jnp.float32),
    )
    joined = jnp.concatenate([query_grad, forget_cot], axis=1)
    summed = lax.psum_scatter(
        lax.dot_general(
            gathered, joined, (((0,), (0,)), ((), ())), preferred_element_type=jnp.float32
        ),
        "fs",
        scatter_dimension=0,
        tiled=True,
    )
    gradients = (summed[:, :col_width], summed[:, col_width:])
    offset = jnp.int32(0)
    results = (
        fold_one(
            empty,
            lax.all_gather(gradients[0].astype(jnp.bfloat16), "fs", axis=0, tiled=True).astype(
                jnp.float32
            ),
            offset,
            row_roots[0],
            gradients[0],
        ),
        fold_one(
            empty,
            lax.all_gather(gradients[1].astype(jnp.bfloat16), "fs", axis=0, tiled=True).astype(
                jnp.float32
            ),
            offset,
            row_roots[1],
            gradients[1],
        ),
    )
    query_trace = jnp.sum(jnp.diagonal(results[0][2], axis1=1, axis2=2))
    forget_trace = jnp.sum(jnp.diagonal(results[1][2], axis1=1, axis2=2))
    query_outer, forget_outer, query_square, forget_square = (
        lax.psum(results[0][1].astype(jnp.bfloat16), "tp").astype(jnp.float32),
        lax.psum(results[1][1].astype(jnp.bfloat16), "tp").astype(jnp.float32),
        lax.psum(query_trace.astype(jnp.bfloat16), "tp").astype(jnp.float32),
        lax.psum(forget_trace.astype(jnp.bfloat16), "tp").astype(jnp.float32),
    )
    query_out = finish(
        query_weight,
        query_moment,
        query_rows,
        query_cols,
        query_col_root,
        results[0][0],
        query_outer,
        results[0][2],
        query_square,
    )
    forget_out = finish(
        forget_weight,
        forget_moment,
        forget_rows,
        forget_cols,
        forget_col_root,
        results[1][0],
        forget_outer,
        results[1][2],
        forget_square,
    )
    return (
        query_out[0],
        forget_out[0],
        query_out[1],
        forget_out[1],
        query_out[2],
        forget_out[2],
        query_out[3],
        forget_out[3],
        query_out[4],
        forget_out[4],
        query_out[5],
        forget_out[5],
    )


def linear_pairs(fs_size, tp_size, target):
    pairs = []
    for f in range(fs_size):
        for t in range(tp_size):
            to_f, to_t = target(f, t)
            pairs.append((f * tp_size + t, to_f * tp_size + to_t))
    return pairs


def gather_operands(keep, send, fs_size, tp_size):
    axes = ("fs", "tp")

    def move(value, target):
        return lax.ppermute(value, axes, linear_pairs(fs_size, tp_size, target))

    def partner(f, t):
        return (f, t ^ 1)

    def first_hop(f, t):
        return (f ^ 1, t) if t % 2 == 0 else (f, t ^ 2)

    def second_hop(f, t):
        return (f, t ^ 2) if t % 2 == 0 else (f ^ 1, t)

    lanes = [jnp.stack([keep, move(send, partner)])]
    for k in range(1, fs_size // 2):
        step = k & -k if k & (k - 1) == 0 else k & (k - 1) ^ k
        source = lanes[k ^ step]
        lanes.append(move(source, lambda f, t, step=step: (f ^ (2 * step), t)))
    sets = []
    nears = []
    for s, lane in enumerate(lanes):
        if s & 1:
            nears.append(move(nears[s ^ 1], lambda f, t: (f ^ 2, t)))
        else:
            nears.append(move(lane, first_hop))
        pair = jnp.stack([lane, nears[s]])
        far = move(pair, second_hop)
        sets.append((pair, far, move(pair, partner), move(far, partner)))
    return sets


def assemble(place, pieces, x_set, y_set, sem):
    odd, upper = place[0], place[1]
    tokens, width = pieces[0].shape[2:]
    own = width // 2
    hidden = y_set.shape[1] // 2

    def copies(x_pieces, y_pieces):
        for p in range(2):
            rows = pl.ds(p * tokens, tokens)
            for h in range(2):
                for c in range(2):
                    col = pl.multiple_of(((upper ^ h) * 2 + c) * width, width)
                    pltpu.make_async_copy(
                        x_pieces[h].at[p, c], x_set.at[rows, pl.ds(col, width)], sem.at[0]
                    ).start()
                    for i in range(2):
                        pltpu.make_async_copy(
                            y_pieces[p].at[h, 1 - c, :, pl.ds(i * own, own)],
                            y_set.at[rows, pl.ds(i * hidden + (2 * h + c) * own, own)],
                            sem.at[1],
                        ).start()

    pair, far, pair_other, far_other = pieces

    @pl.when(odd == 0)
    def _():
        copies((pair, far), (pair_other, far_other))

    @pl.when(odd == 1)
    def _():
        copies((pair_other, far_other), (pair, far))


def assembled(x_set, y_set, sem):
    for k, whole in enumerate((x_set, y_set)):
        pltpu.make_async_copy(whole, whole, sem.at[k]).wait()


def product(x_set, y_set, cols):
    return lax.dot_general(
        x_set[...], y_set[:, cols], (((0,), (0,)), ((), ())), preferred_element_type=jnp.float32
    )


def sum_kernel(first, n_fetched, place, *refs):
    pieces, refs = refs[:4], refs[4:]
    if not first:
        refs = refs[1:]
    sources, refs = refs[:n_fetched], refs[n_fetched:]
    acc, fetched, (x_set, y_set, sem, fetch_sem) = refs[0], refs[1:-4], refs[-4:]
    assemble(place, pieces, x_set, y_set, sem)
    copies = [
        pltpu.make_async_copy(src, dst, fetch_sem.at[j])
        for j, (src, dst) in enumerate(zip(sources, fetched, strict=True))
    ]
    assembled(x_set, y_set, sem)
    for copy in copies:
        copy.start()
    total, chunk = acc.shape[1], x_set.shape[0]
    for at in range(0, total, chunk):
        cols = slice(at, at + chunk)
        part = product(x_set, y_set, cols)
        acc[:, cols] = part if first else acc[:, cols] + part
    for copy in copies:
        copy.wait()


def tail_kernel(place, *refs):
    pieces, acc, refs = refs[:4], refs[4], refs[5:]
    sides = [refs[6 * i : 6 * i + 6] for i in range(2)]
    refs = refs[12:]
    outs = [refs[6 * i : 6 * i + 6] for i in range(2)]
    refs = refs[12:]
    x_set, y_set, grad, sem, store_sem = refs[:5]
    made = [refs[5 + 6 * i : 11 + 6 * i] for i in range(2)]
    odd, band = place[0], place[2]
    model, total = grad.shape
    hidden = total // 2
    own = pieces[0].shape[3] // 2
    rows_here = sides[0][0].shape[0]

    assemble(place, pieces, x_set, y_set, sem)
    assembled(x_set, y_set, sem)

    chunk = x_set.shape[0]
    squares = [jnp.zeros((8, chunk), jnp.float32)] * 2
    for at in range(0, total, chunk):
        cols = slice(at, at + chunk)
        part = acc[:, cols] + product(x_set, y_set, cols)
        grad[:, cols] = part.astype(jnp.bfloat16)
        squares[at // hidden] += jnp.sum((part * part).reshape(-1, 8, chunk), axis=0)

    stores = []

    def store(src, dst, at):
        stores.append(pltpu.make_async_copy(src, dst, store_sem.at[at]))
        stores[-1].start()

    scales = []
    for i in range(2):
        _, row_root, weight, moment, cols, col_root = sides[i]
        results, cols_next = made[i][:4], made[i][5]
        square = jnp.sum(squares[i], keepdims=True)
        scale = jnp.sqrt(model * hidden / (square + 1.0))
        scales.append(scale)
        mine = pl.multiple_of(i * hidden + odd * own, own)
        own_grad = grad[:, pl.ds(mine, own)]
        left = jnp.dot(row_root[...], own_grad, preferred_element_type=jnp.float32)
        left_high = left.astype(jnp.bfloat16)
        left_low = (left - left_high.astype(jnp.float32)).astype(jnp.bfloat16)
        column_total = lax.dot_general(
            own_grad, own_grad, (((0,), (0,)), ((), ())), preferred_element_type=jnp.float32
        )
        for h in range(own // HEAD):
            at = slice(h * HEAD, (h + 1) * HEAD)
            cols_next[h] = (
                stat_decay * cols[h]
                + (1.0 - stat_decay) / model * scale * scale * column_total[at, at]
            )
            root = col_root[h]
            precond = scale * (
                jnp.dot(left_high[:, at], root, preferred_element_type=jnp.float32)
                + jnp.dot(left_low[:, at], root, preferred_element_type=jnp.float32)
            )
            moment_next = moment_decay * moment[:, at] + (1.0 - moment_decay) * precond
            update_step = moment_decay * moment_next + (1.0 - moment_decay) * precond
            master = weight[:, at] - learn_rate * update_step
            for to, value in zip(
                results,
                (master, master.astype(jnp.bfloat16), update_step, moment_next),
                strict=True,
            ):
                to[:, at] = value
        for j, src in enumerate(results):
            store(src, outs[i][j], (i, j))
        store(cols_next, outs[i][5], (i, 4))
    first = pl.multiple_of(band * rows_here, rows_here)
    piece = 2 * own
    for i in range(2):
        rows, rows_next = sides[i][0], made[i][4]
        band_grad = grad[pl.ds(first, rows_here), i * hidden : (i + 1) * hidden]
        factor = (1.0 - stat_decay) / hidden * scales[i] * scales[i]
        for k in range(model // piece):
            at = slice(k * piece, (k + 1) * piece)
            part = lax.dot_general(
                band_grad,
                grad[at, i * hidden : (i + 1) * hidden],
                (((1,), (1,)), ((), ())),
                preferred_element_type=jnp.float32,
            )
            rows_next[:, at] = stat_decay * rows[:, at] + factor * part
            store(rows_next.at[:, at], outs[i][4].at[:, at], (i, 5 + k))
    for copy in stores:
        copy.wait()


def prepare_kernel(place, *refs):
    sources, (keep, send), held, sem = refs[:5], refs[5:7], refs[7:12], refs[12]
    copies = [
        pltpu.make_async_copy(src, dst, sem.at[j])
        for j, (src, dst) in enumerate(zip(sources, held, strict=True))
    ]
    for copy in copies:
        copy.start()
    for copy in copies:
        copy.wait()
    inputs, query_grad, forget_grad, forget_pre, lower_bound = held
    own = query_grad.shape[1]
    sigma_gate = jax.nn.sigmoid(forget_pre[...].astype(jnp.float32))
    forget_cot = (
        forget_grad[...].astype(jnp.float32)
        * (1.0 - lower_bound[...])
        * sigma_gate
        * (1.0 - sigma_gate)
    ).astype(jnp.bfloat16)

    def write(x_to, y_to):
        x_to[...] = inputs[...]
        y_to[:, :own] = query_grad[...]
        y_to[:, own:] = forget_cot

    @pl.when(place[0] == 0)
    def _():
        write(keep, send)

    @pl.when(place[0] == 1)
    def _():
        write(send, keep)


def gathered_plan(
    inputs,
    query_grad,
    forget_grad,
    forget_pre,
    lower_bound,
    query_weight,
    forget_weight,
    query_moment,
    forget_moment,
    query_rows,
    forget_rows,
    query_cols,
    forget_cols,
    query_row_root,
    forget_row_root,
    query_col_root,
    forget_col_root,
    fs_size,
    tp_size,
):
    tp_at = lax.axis_index("tp")
    place = jnp.stack([tp_at & 1, tp_at >> 1, lax.axis_index("fs")]).astype(jnp.int32)
    smem = pl.BlockSpec(memory_space=pltpu.SMEM)
    vmem = pl.BlockSpec(memory_space=pltpu.VMEM)
    params = pltpu.CompilerParams(vmem_limit_bytes=21 * 2**20)
    hbm = pl.BlockSpec(memory_space=pltpu.HBM)
    saved = (inputs, query_grad, forget_grad, forget_pre, lower_bound[None])
    keep, send = pl.pallas_call(
        prepare_kernel,
        out_shape=(pltpu.VMEM(inputs.shape, inputs.dtype),) * 2,
        in_specs=[smem] + [hbm] * 5,
        out_specs=[vmem] * 2,
        scratch_shapes=[pltpu.VMEM(v.shape, v.dtype) for v in saved]
        + [pltpu.SemaphoreType.DMA((5,))],
        compiler_params=params,
        name="prepare",
    )(place, *(pltpu.with_memory_space_constraint(v, pltpu.HBM) for v in saved))
    sets = gather_operands(keep, send, fs_size, tp_size)
    model = inputs.shape[1] * tp_size
    total = 2 * query_grad.shape[1] * tp_size
    sides = (
        (query_rows, query_row_root, query_weight, query_moment, query_cols, query_col_root),
        (forget_rows, forget_row_root, forget_weight, forget_moment, forget_cols, forget_col_root),
    )
    wide = jax.ShapeDtypeStruct(query_weight.shape, jnp.float32)
    narrow = jax.ShapeDtypeStruct(query_weight.shape, jnp.bfloat16)
    row_kind = jax.ShapeDtypeStruct(query_rows.shape, jnp.float32)
    col_kind = jax.ShapeDtypeStruct(query_cols.shape, jnp.float32)
    kinds = (wide, narrow, wide, wide, row_kind, col_kind)
    held = [pltpu.VMEM(k.shape, k.dtype) for k in kinds * 2]
    anywhere = pl.BlockSpec(memory_space=pl.ANY)
    set_scratch = [
        pltpu.VMEM((2 * inputs.shape[0], model), jnp.bfloat16),
        pltpu.VMEM((2 * inputs.shape[0], total), jnp.bfloat16),
    ]
    wanted = [[side[0] for side in sides], [v for side in sides for v in side[1:]]]
    wanted += [[]] * (len(sets) - 3)
    acc, fetched = [], []
    for s, pieces in enumerate(sets[:-1]):
        fetch = [pltpu.with_memory_space_constraint(v, pltpu.HBM) for v in wanted[s]]
        made = pl.pallas_call(
            partial(sum_kernel, not acc, len(fetch)),
            out_shape=[pltpu.VMEM((model, total), jnp.float32)]
            + [pltpu.VMEM(v.shape, v.dtype) for v in fetch],
            in_specs=[smem] + [anywhere] * 4 + [vmem] * len(acc) + [hbm] * len(fetch),
            out_specs=[vmem] * (1 + len(fetch)),
            scratch_shapes=set_scratch
            + [pltpu.SemaphoreType.DMA((2,)), pltpu.SemaphoreType.DMA((max(len(fetch), 1),))],
            input_output_aliases={5: 0} if acc else {},
            compiler_params=pltpu.CompilerParams(vmem_limit_bytes=12 * 2**20),
        )(place, *pieces, *acc, *fetch)
        acc, fetched = made[:1], fetched + list(made[1:])
    half = len(fetched[2:]) // 2
    loaded = [fetched[0], *fetched[2 : 2 + half], fetched[1], *fetched[2 + half :]]
    operands = [*sets[-1], pltpu.with_memory_space_constraint(*acc, pltpu.VMEM)]
    operands += [pltpu.with_memory_space_constraint(v, pltpu.VMEM) for v in loaded]
    out = pl.pallas_call(
        tail_kernel,
        out_shape=kinds * 2,
        in_specs=[smem] + [anywhere] * 4 + [vmem] * 13,
        out_specs=[hbm] * 12,
        scratch_shapes=set_scratch
        + [
            pltpu.VMEM((model, total), jnp.bfloat16),
            pltpu.SemaphoreType.DMA((2,)),
            pltpu.SemaphoreType.DMA((2, 5 + model // query_weight.shape[1] // 2)),
        ]
        + held,
        compiler_params=params,
        name="tail",
    )(place, *operands)
    return tuple(v for both in zip(out[:6], out[6:], strict=True) for v in both)


def use_gathered(tokens, model, hidden, fs_size, tp_size):
    blocks = fs_size // 2
    square_grid = tp_size == 4 and fs_size % 2 == 0 and blocks & (blocks - 1) == 0
    return square_grid and tokens * (model + 2 * hidden) <= model * 2 * hidden


def on_device(fs_size, tp_size, inputs, query_grad, forget_grad, forget_pre, lower_bound, *rest):
    tokens = inputs.shape[0] * fs_size
    if use_gathered(tokens, inputs.shape[1] * tp_size, query_grad.shape[1] * tp_size, fs_size, tp_size):
        return gathered_plan(
            inputs, query_grad, forget_grad, forget_pre, lower_bound, *rest, fs_size, tp_size
        )
    sigma_gate = jax.nn.sigmoid(forget_pre.astype(jnp.float32))
    forget_cot = (
        forget_grad.astype(jnp.float32) * (1.0 - lower_bound) * sigma_gate * (1.0 - sigma_gate)
    ).astype(jnp.bfloat16)
    return summed_plan(inputs, query_grad, forget_cot, *rest)


def solution(mesh):
    in_specs = (
        P("fs", "tp"),
        P("fs", "tp"),
        P("fs", "tp"),
        P("fs", "tp"),
        P("tp"),
        P("fs", "tp"),
        P("fs", "tp"),
        P("fs", "tp"),
        P("fs", "tp"),
        P("fs", None),
        P("fs", None),
        P("tp", None, None),
        P("tp", None, None),
        P("fs", None),
        P("fs", None),
        P("tp", None, None),
        P("tp", None, None),
    )
    out_specs = (
        P("fs", "tp"),
        P("fs", "tp"),
        P("fs", "tp"),
        P("fs", "tp"),
        P("fs", "tp"),
        P("fs", "tp"),
        P("fs", "tp"),
        P("fs", "tp"),
        P("fs", None),
        P("fs", None),
        P("tp", None, None),
        P("tp", None, None),
    )
    sizes = (mesh.shape["fs"], mesh.shape["tp"])
    return jax.shard_map(
        partial(on_device, *sizes), mesh=mesh, in_specs=in_specs, out_specs=out_specs, check_vma=False
    )
```

```python
from functools import partial

import jax
import jax.numpy as jnp
from jax import lax
from jax.experimental import pallas as pl
from jax.experimental.pallas import tpu as pltpu
from jax.sharding import PartitionSpec as P


D = 2048
HW = 1024
HEAD = 128


stat_decay = 0.9
moment_decay = 0.9
learn_rate = 0.02
highest = lax.Precision.HIGHEST


def fold_one(carry_state, shard_piece, offset, root_mine, grad_mine):
    left_sum, outer_rows, column_total = carry_state
    row_count, col_width = shard_piece.shape
    left_sum = left_sum + jnp.dot(root_mine, shard_piece, precision=highest)
    outer_piece = lax.dot_general(
        grad_mine, shard_piece, (((1,), (1,)), ((), ())), precision=highest
    )
    outer_rows = lax.dynamic_update_slice_in_dim(outer_rows, outer_piece, offset, 1)
    by_head = shard_piece.reshape(row_count, col_width // HEAD, HEAD)
    column_total = column_total + jnp.einsum("rhi,rhj->hij", by_head, by_head, precision=highest)
    return (left_sum, outer_rows, column_total)


def finish(weight, moment, rows, cols, col_root, left_sum, outer_rows, column_total, square):
    norm_scale = jnp.sqrt(D * HW / (square + 1.0))
    scale_twice = norm_scale * norm_scale
    rows_next = stat_decay * rows + (1.0 - stat_decay) / HW * scale_twice * outer_rows
    cols_next = stat_decay * cols + (1.0 - stat_decay) / D * scale_twice * column_total
    shard_rows, col_width = left_sum.shape
    shaped = left_sum.reshape(shard_rows, col_width // HEAD, HEAD)
    precond = norm_scale * jnp.einsum(
        "rhi,hij->rhj", shaped, col_root.astype(jnp.float32), precision=highest
    ).reshape(shard_rows, col_width)
    moment_next = moment_decay * moment + (1.0 - moment_decay) * precond
    update_step = moment_decay * moment_next + (1.0 - moment_decay) * precond
    master = weight - learn_rate * update_step
    return (master, master.astype(jnp.bfloat16), update_step, moment_next, rows_next, cols_next)


def summed_plan(
    inputs,
    query_grad,
    forget_cot,
    query_weight,
    forget_weight,
    query_moment,
    forget_moment,
    query_rows,
    forget_rows,
    query_cols,
    forget_cols,
    query_row_root,
    forget_row_root,
    query_col_root,
    forget_col_root,
):
    gathered = lax.all_gather(inputs, "tp", axis=1, tiled=True)
    shard_rows, col_width = query_weight.shape
    heads_here = col_width // HEAD
    row_roots = (query_row_root.astype(jnp.float32), forget_row_root.astype(jnp.float32))
    empty = (
        jnp.zeros((shard_rows, col_width), jnp.float32),
        jnp.zeros((shard_rows, D), jnp.float32),
        jnp.zeros((heads_here, HEAD, HEAD), jnp.float32),
    )
    joined = jnp.concatenate([query_grad, forget_cot], axis=1)
    summed = lax.psum_scatter(
        lax.dot_general(
            gathered, joined, (((0,), (0,)), ((), ())), preferred_element_type=jnp.float32
        ),
        "fs",
        scatter_dimension=0,
        tiled=True,
    )
    gradients = (summed[:, :col_width], summed[:, col_width:])
    offset = jnp.int32(0)
    results = (
        fold_one(
            empty,
            lax.all_gather(gradients[0].astype(jnp.bfloat16), "fs", axis=0, tiled=True).astype(
                jnp.float32
            ),
            offset,
            row_roots[0],
            gradients[0],
        ),
        fold_one(
            empty,
            lax.all_gather(gradients[1].astype(jnp.bfloat16), "fs", axis=0, tiled=True).astype(
                jnp.float32
            ),
            offset,
            row_roots[1],
            gradients[1],
        ),
    )
    query_trace = jnp.sum(jnp.diagonal(results[0][2], axis1=1, axis2=2))
    forget_trace = jnp.sum(jnp.diagonal(results[1][2], axis1=1, axis2=2))
    query_outer, forget_outer, query_square, forget_square = (
        lax.psum(results[0][1].astype(jnp.bfloat16), "tp").astype(jnp.float32),
        lax.psum(results[1][1].astype(jnp.bfloat16), "tp").astype(jnp.float32),
        lax.psum(query_trace.astype(jnp.bfloat16), "tp").astype(jnp.float32),
        lax.psum(forget_trace.astype(jnp.bfloat16), "tp").astype(jnp.float32),
    )
    query_out = finish(
        query_weight,
        query_moment,
        query_rows,
        query_cols,
        query_col_root,
        results[0][0],
        query_outer,
        results[0][2],
        query_square,
    )
    forget_out = finish(
        forget_weight,
        forget_moment,
        forget_rows,
        forget_cols,
        forget_col_root,
        results[1][0],
        forget_outer,
        results[1][2],
        forget_square,
    )
    return (
        query_out[0],
        forget_out[0],
        query_out[1],
        forget_out[1],
        query_out[2],
        forget_out[2],
        query_out[3],
        forget_out[3],
        query_out[4],
        forget_out[4],
        query_out[5],
        forget_out[5],
    )


def linear_pairs(fs_size, tp_size, target):
    pairs = []
    for f in range(fs_size):
        for t in range(tp_size):
            to_f, to_t = target(f, t)
            pairs.append((f * tp_size + t, to_f * tp_size + to_t))
    return pairs


def gather_operands(keep, send, fs_size, tp_size):
    axes = ("fs", "tp")

    def move(value, target):
        return lax.ppermute(value, axes, linear_pairs(fs_size, tp_size, target))

    def partner(f, t):
        return (f, t ^ 1)

    def first_hop(f, t):
        return (f ^ 1, t) if t % 2 == 0 else (f, t ^ 2)

    def second_hop(f, t):
        return (f, t ^ 2) if t % 2 == 0 else (f ^ 1, t)

    lanes = [jnp.stack([keep, move(send, partner)])]
    for k in range(1, fs_size // 2):
        step = k & -k if k & (k - 1) == 0 else k & (k - 1) ^ k
        source = lanes[k ^ step]
        lanes.append(move(source, lambda f, t, step=step: (f ^ (2 * step), t)))
    sets = []
    nears = []
    for s, lane in enumerate(lanes):
        if s & 1:
            nears.append(move(nears[s ^ 1], lambda f, t: (f ^ 2, t)))
        else:
            nears.append(move(lane, first_hop))
        pair = jnp.stack([lane, nears[s]])
        far = move(pair, second_hop)
        sets.append((pair, far, move(pair, partner), move(far, partner)))
    return sets


def assemble(place, pieces, x_set, y_set, sem):
    odd, upper = place[0], place[1]
    tokens, width = pieces[0].shape[2:]
    own = width // 2
    hidden = y_set.shape[1] // 2

    def copies(x_pieces, y_pieces):
        for p in range(2):
            rows = pl.ds(p * tokens, tokens)
            for h in range(2):
                for c in range(2):
                    col = pl.multiple_of(((upper ^ h) * 2 + c) * width, width)
                    pltpu.make_async_copy(
                        x_pieces[h].at[p, c], x_set.at[rows, pl.ds(col, width)], sem.at[0]
                    ).start()
                    for i in range(2):
                        pltpu.make_async_copy(
                            y_pieces[p].at[h, 1 - c, :, pl.ds(i * own, own)],
                            y_set.at[rows, pl.ds(i * hidden + (2 * h + c) * own, own)],
                            sem.at[1],
                        ).start()

    pair, far, pair_other, far_other = pieces

    @pl.when(odd == 0)
    def _():
        copies((pair, far), (pair_other, far_other))

    @pl.when(odd == 1)
    def _():
        copies((pair_other, far_other), (pair, far))


def assembled(x_set, y_set, sem):
    for k, whole in enumerate((x_set, y_set)):
        pltpu.make_async_copy(whole, whole, sem.at[k]).wait()


def product(x_set, y_set, cols):
    return lax.dot_general(
        x_set[...], y_set[:, cols], (((0,), (0,)), ((), ())), preferred_element_type=jnp.float32
    )


def sum_kernel(first, n_fetched, place, *refs):
    pieces, refs = refs[:4], refs[4:]
    if not first:
        refs = refs[1:]
    sources, refs = refs[:n_fetched], refs[n_fetched:]
    acc, fetched, (x_set, y_set, sem, fetch_sem) = refs[0], refs[1:-4], refs[-4:]
    assemble(place, pieces, x_set, y_set, sem)
    copies = [
        pltpu.make_async_copy(src, dst, fetch_sem.at[j])
        for j, (src, dst) in enumerate(zip(sources, fetched, strict=True))
    ]
    assembled(x_set, y_set, sem)
    for copy in copies:
        copy.start()
    total, chunk = acc.shape[1], x_set.shape[0]
    for at in range(0, total, chunk):
        cols = slice(at, at + chunk)
        part = product(x_set, y_set, cols)
        acc[:, cols] = part if first else acc[:, cols] + part
    for copy in copies:
        copy.wait()


def tail_kernel(place, *refs):
    pieces, acc, refs = refs[:4], refs[4], refs[5:]
    sides = [refs[6 * i : 6 * i + 6] for i in range(2)]
    refs = refs[12:]
    outs = [refs[6 * i : 6 * i + 6] for i in range(2)]
    refs = refs[12:]
    x_set, y_set, grad, roots, sem, store_sem = refs[:6]
    made = [refs[6 + 6 * i : 12 + 6 * i] for i in range(2)]
    odd, band = place[0], place[2]
    model, total = grad.shape
    hidden = total // 2
    own = pieces[0].shape[3] // 2
    rows_here = sides[0][0].shape[0]

    assemble(place, pieces, x_set, y_set, sem)
    roots[...] = jnp.zeros(roots.shape, roots.dtype)
    for i in range(2):
        for k in range(2):
            for h in range(own // HEAD):
                at = slice(h * HEAD, (h + 1) * HEAD)
                roots[i, k * own + h * HEAD : k * own + (h + 1) * HEAD, at] = sides[i][5][h]
    assembled(x_set, y_set, sem)

    chunk = x_set.shape[0]
    squares = [jnp.zeros((8, chunk), jnp.float32)] * 2
    for at in range(0, total, chunk):
        cols = slice(at, at + chunk)
        part = acc[:, cols] + product(x_set, y_set, cols)
        grad[:, cols] = part.astype(jnp.bfloat16)
        squares[at // hidden] += jnp.sum((part * part).reshape(-1, 8, chunk), axis=0)

    stores = []

    def store(src, dst, at):
        stores.append(pltpu.make_async_copy(src, dst, store_sem.at[at]))
        stores[-1].start()

    scales = []
    for i in range(2):
        _, row_root, weight, moment, cols, _ = sides[i]
        results, cols_next = made[i][:4], made[i][5]
        square = jnp.sum(squares[i], keepdims=True)
        scale = jnp.sqrt(model * hidden / (square + 1.0))
        scales.append(scale)
        mine = pl.multiple_of(i * hidden + odd * own, own)
        own_grad = grad[:, pl.ds(mine, own)]
        left = jnp.dot(row_root[...], own_grad, preferred_element_type=jnp.float32)
        left_high = left.astype(jnp.bfloat16)
        left_low = (left - left_high.astype(jnp.float32)).astype(jnp.bfloat16)
        column_total = lax.dot_general(
            own_grad, own_grad, (((0,), (0,)), ((), ())), preferred_element_type=jnp.float32
        )
        for h in range(own // HEAD):
            at = slice(h * HEAD, (h + 1) * HEAD)
            cols_next[h] = (
                stat_decay * cols[h]
                + (1.0 - stat_decay) / model * scale * scale * column_total[at, at]
            )
        precond = scale * jnp.dot(
            jnp.concatenate([left_high, left_low], axis=1),
            roots[i],
            preferred_element_type=jnp.float32,
        )
        moment_next = moment_decay * moment[...] + (1.0 - moment_decay) * precond
        update_step = moment_decay * moment_next + (1.0 - moment_decay) * precond
        master = weight[...] - learn_rate * update_step
        for to, value in zip(
            results, (master, master.astype(jnp.bfloat16), update_step, moment_next), strict=True
        ):
            to[...] = value
        for j, src in enumerate(results):
            store(src, outs[i][j], (i, j))
        store(cols_next, outs[i][5], (i, 4))
    first = pl.multiple_of(band * rows_here, rows_here)
    piece = 2 * own
    for i in range(2):
        rows, rows_next = sides[i][0], made[i][4]
        band_grad = grad[pl.ds(first, rows_here), i * hidden : (i + 1) * hidden]
        factor = (1.0 - stat_decay) / hidden * scales[i] * scales[i]
        for k in range(model // piece):
            at = slice(k * piece, (k + 1) * piece)
            part = lax.dot_general(
                band_grad,
                grad[at, i * hidden : (i + 1) * hidden],
                (((1,), (1,)), ((), ())),
                preferred_element_type=jnp.float32,
            )
            rows_next[:, at] = stat_decay * rows[:, at] + factor * part
            store(rows_next.at[:, at], outs[i][4].at[:, at], (i, 5 + k))
    for copy in stores:
        copy.wait()


def prepare_kernel(place, *refs):
    sources, (keep, send), held, sem = refs[:5], refs[5:7], refs[7:12], refs[12]
    copies = [
        pltpu.make_async_copy(src, dst, sem.at[j])
        for j, (src, dst) in enumerate(zip(sources, held, strict=True))
    ]
    for copy in copies:
        copy.start()
    for copy in copies:
        copy.wait()
    inputs, query_grad, forget_grad, forget_pre, lower_bound = held
    own = query_grad.shape[1]
    sigma_gate = jax.nn.sigmoid(forget_pre[...].astype(jnp.float32))
    forget_cot = (
        forget_grad[...].astype(jnp.float32)
        * (1.0 - lower_bound[...])
        * sigma_gate
        * (1.0 - sigma_gate)
    ).astype(jnp.bfloat16)

    def write(x_to, y_to):
        x_to[...] = inputs[...]
        y_to[:, :own] = query_grad[...]
        y_to[:, own:] = forget_cot

    @pl.when(place[0] == 0)
    def _():
        write(keep, send)

    @pl.when(place[0] == 1)
    def _():
        write(send, keep)


def gathered_plan(
    inputs,
    query_grad,
    forget_grad,
    forget_pre,
    lower_bound,
    query_weight,
    forget_weight,
    query_moment,
    forget_moment,
    query_rows,
    forget_rows,
    query_cols,
    forget_cols,
    query_row_root,
    forget_row_root,
    query_col_root,
    forget_col_root,
    fs_size,
    tp_size,
):
    tp_at = lax.axis_index("tp")
    place = jnp.stack([tp_at & 1, tp_at >> 1, lax.axis_index("fs")]).astype(jnp.int32)
    smem = pl.BlockSpec(memory_space=pltpu.SMEM)
    vmem = pl.BlockSpec(memory_space=pltpu.VMEM)
    params = pltpu.CompilerParams(vmem_limit_bytes=21 * 2**20)
    hbm = pl.BlockSpec(memory_space=pltpu.HBM)
    saved = (inputs, query_grad, forget_grad, forget_pre, lower_bound[None])
    keep, send = pl.pallas_call(
        prepare_kernel,
        out_shape=(pltpu.VMEM(inputs.shape, inputs.dtype),) * 2,
        in_specs=[smem] + [hbm] * 5,
        out_specs=[vmem] * 2,
        scratch_shapes=[pltpu.VMEM(v.shape, v.dtype) for v in saved]
        + [pltpu.SemaphoreType.DMA((5,))],
        compiler_params=params,
        name="prepare",
    )(place, *(pltpu.with_memory_space_constraint(v, pltpu.HBM) for v in saved))
    sets = gather_operands(keep, send, fs_size, tp_size)
    model = inputs.shape[1] * tp_size
    total = 2 * query_grad.shape[1] * tp_size
    sides = (
        (query_rows, query_row_root, query_weight, query_moment, query_cols, query_col_root),
        (forget_rows, forget_row_root, forget_weight, forget_moment, forget_cols, forget_col_root),
    )
    wide = jax.ShapeDtypeStruct(query_weight.shape, jnp.float32)
    narrow = jax.ShapeDtypeStruct(query_weight.shape, jnp.bfloat16)
    row_kind = jax.ShapeDtypeStruct(query_rows.shape, jnp.float32)
    col_kind = jax.ShapeDtypeStruct(query_cols.shape, jnp.float32)
    kinds = (wide, narrow, wide, wide, row_kind, col_kind)
    held = [pltpu.VMEM(k.shape, k.dtype) for k in kinds * 2]
    anywhere = pl.BlockSpec(memory_space=pl.ANY)
    set_scratch = [
        pltpu.VMEM((2 * inputs.shape[0], model), jnp.bfloat16),
        pltpu.VMEM((2 * inputs.shape[0], total), jnp.bfloat16),
    ]
    wanted = [[side[0] for side in sides], [v for side in sides for v in side[1:]]]
    wanted += [[]] * (len(sets) - 3)
    acc, fetched = [], []
    for s, pieces in enumerate(sets[:-1]):
        fetch = [pltpu.with_memory_space_constraint(v, pltpu.HBM) for v in wanted[s]]
        made = pl.pallas_call(
            partial(sum_kernel, not acc, len(fetch)),
            out_shape=[pltpu.VMEM((model, total), jnp.float32)]
            + [pltpu.VMEM(v.shape, v.dtype) for v in fetch],
            in_specs=[smem] + [anywhere] * 4 + [vmem] * len(acc) + [hbm] * len(fetch),
            out_specs=[vmem] * (1 + len(fetch)),
            scratch_shapes=set_scratch
            + [pltpu.SemaphoreType.DMA((2,)), pltpu.SemaphoreType.DMA((max(len(fetch), 1),))],
            input_output_aliases={5: 0} if acc else {},
            compiler_params=pltpu.CompilerParams(vmem_limit_bytes=12 * 2**20),
        )(place, *pieces, *acc, *fetch)
        acc, fetched = made[:1], fetched + list(made[1:])
    half = len(fetched[2:]) // 2
    loaded = [fetched[0], *fetched[2 : 2 + half], fetched[1], *fetched[2 + half :]]
    operands = [*sets[-1], pltpu.with_memory_space_constraint(*acc, pltpu.VMEM)]
    operands += [pltpu.with_memory_space_constraint(v, pltpu.VMEM) for v in loaded]
    out = pl.pallas_call(
        tail_kernel,
        out_shape=kinds * 2,
        in_specs=[smem] + [anywhere] * 4 + [vmem] * 13,
        out_specs=[hbm] * 12,
        scratch_shapes=set_scratch
        + [
            pltpu.VMEM((model, total), jnp.bfloat16),
            pltpu.VMEM((2, 2 * query_weight.shape[1], query_weight.shape[1]), jnp.bfloat16),
            pltpu.SemaphoreType.DMA((2,)),
            pltpu.SemaphoreType.DMA((2, 5 + model // query_weight.shape[1] // 2)),
        ]
        + held,
        compiler_params=params,
        name="tail",
    )(place, *operands)
    return tuple(v for both in zip(out[:6], out[6:], strict=True) for v in both)


def use_gathered(tokens, model, hidden, fs_size, tp_size):
    blocks = fs_size // 2
    square_grid = tp_size == 4 and fs_size % 2 == 0 and blocks & (blocks - 1) == 0
    return square_grid and tokens * (model + 2 * hidden) <= model * 2 * hidden


def on_device(fs_size, tp_size, inputs, query_grad, forget_grad, forget_pre, lower_bound, *rest):
    tokens = inputs.shape[0] * fs_size
    if use_gathered(tokens, inputs.shape[1] * tp_size, query_grad.shape[1] * tp_size, fs_size, tp_size):
        return gathered_plan(
            inputs, query_grad, forget_grad, forget_pre, lower_bound, *rest, fs_size, tp_size
        )
    sigma_gate = jax.nn.sigmoid(forget_pre.astype(jnp.float32))
    forget_cot = (
        forget_grad.astype(jnp.float32) * (1.0 - lower_bound) * sigma_gate * (1.0 - sigma_gate)
    ).astype(jnp.bfloat16)
    return summed_plan(inputs, query_grad, forget_cot, *rest)


def solution(mesh):
    in_specs = (
        P("fs", "tp"),
        P("fs", "tp"),
        P("fs", "tp"),
        P("fs", "tp"),
        P("tp"),
        P("fs", "tp"),
        P("fs", "tp"),
        P("fs", "tp"),
        P("fs", "tp"),
        P("fs", None),
        P("fs", None),
        P("tp", None, None),
        P("tp", None, None),
        P("fs", None),
        P("fs", None),
        P("tp", None, None),
        P("tp", None, None),
    )
    out_specs = (
        P("fs", "tp"),
        P("fs", "tp"),
        P("fs", "tp"),
        P("fs", "tp"),
        P("fs", "tp"),
        P("fs", "tp"),
        P("fs", "tp"),
        P("fs", "tp"),
        P("fs", None),
        P("fs", None),
        P("tp", None, None),
        P("tp", None, None),
    )
    sizes = (mesh.shape["fs"], mesh.shape["tp"])
    return jax.shard_map(
        partial(on_device, *sizes), mesh=mesh, in_specs=in_specs, out_specs=out_specs, check_vma=False
    )
```

```python
from functools import partial

import jax
import jax.numpy as jnp
from jax import lax
from jax.experimental import pallas as pl
from jax.experimental.pallas import tpu as pltpu
from jax.sharding import PartitionSpec as P


D = 2048
HW = 1024
HEAD = 128


stat_decay = 0.9
moment_decay = 0.9
learn_rate = 0.02
highest = lax.Precision.HIGHEST


def fold_one(carry_state, shard_piece, offset, root_mine, grad_mine):
    left_sum, outer_rows, column_total = carry_state
    row_count, col_width = shard_piece.shape
    left_sum = left_sum + jnp.dot(root_mine, shard_piece, precision=highest)
    outer_piece = lax.dot_general(
        grad_mine, shard_piece, (((1,), (1,)), ((), ())), precision=highest
    )
    outer_rows = lax.dynamic_update_slice_in_dim(outer_rows, outer_piece, offset, 1)
    by_head = shard_piece.reshape(row_count, col_width // HEAD, HEAD)
    column_total = column_total + jnp.einsum("rhi,rhj->hij", by_head, by_head, precision=highest)
    return (left_sum, outer_rows, column_total)


def finish(weight, moment, rows, cols, col_root, left_sum, outer_rows, column_total, square):
    norm_scale = jnp.sqrt(D * HW / (square + 1.0))
    scale_twice = norm_scale * norm_scale
    rows_next = stat_decay * rows + (1.0 - stat_decay) / HW * scale_twice * outer_rows
    cols_next = stat_decay * cols + (1.0 - stat_decay) / D * scale_twice * column_total
    shard_rows, col_width = left_sum.shape
    shaped = left_sum.reshape(shard_rows, col_width // HEAD, HEAD)
    precond = norm_scale * jnp.einsum(
        "rhi,hij->rhj", shaped, col_root.astype(jnp.float32), precision=highest
    ).reshape(shard_rows, col_width)
    moment_next = moment_decay * moment + (1.0 - moment_decay) * precond
    update_step = moment_decay * moment_next + (1.0 - moment_decay) * precond
    master = weight - learn_rate * update_step
    return (master, master.astype(jnp.bfloat16), update_step, moment_next, rows_next, cols_next)


def summed_plan(
    inputs,
    query_grad,
    forget_cot,
    query_weight,
    forget_weight,
    query_moment,
    forget_moment,
    query_rows,
    forget_rows,
    query_cols,
    forget_cols,
    query_row_root,
    forget_row_root,
    query_col_root,
    forget_col_root,
):
    gathered = lax.all_gather(inputs, "tp", axis=1, tiled=True)
    shard_rows, col_width = query_weight.shape
    heads_here = col_width // HEAD
    row_roots = (query_row_root.astype(jnp.float32), forget_row_root.astype(jnp.float32))
    empty = (
        jnp.zeros((shard_rows, col_width), jnp.float32),
        jnp.zeros((shard_rows, D), jnp.float32),
        jnp.zeros((heads_here, HEAD, HEAD), jnp.float32),
    )
    joined = jnp.concatenate([query_grad, forget_cot], axis=1)
    summed = lax.psum_scatter(
        lax.dot_general(
            gathered, joined, (((0,), (0,)), ((), ())), preferred_element_type=jnp.float32
        ),
        "fs",
        scatter_dimension=0,
        tiled=True,
    )
    gradients = (summed[:, :col_width], summed[:, col_width:])
    offset = jnp.int32(0)
    results = (
        fold_one(
            empty,
            lax.all_gather(gradients[0].astype(jnp.bfloat16), "fs", axis=0, tiled=True).astype(
                jnp.float32
            ),
            offset,
            row_roots[0],
            gradients[0],
        ),
        fold_one(
            empty,
            lax.all_gather(gradients[1].astype(jnp.bfloat16), "fs", axis=0, tiled=True).astype(
                jnp.float32
            ),
            offset,
            row_roots[1],
            gradients[1],
        ),
    )
    query_trace = jnp.sum(jnp.diagonal(results[0][2], axis1=1, axis2=2))
    forget_trace = jnp.sum(jnp.diagonal(results[1][2], axis1=1, axis2=2))
    query_outer, forget_outer, query_square, forget_square = (
        lax.psum(results[0][1].astype(jnp.bfloat16), "tp").astype(jnp.float32),
        lax.psum(results[1][1].astype(jnp.bfloat16), "tp").astype(jnp.float32),
        lax.psum(query_trace.astype(jnp.bfloat16), "tp").astype(jnp.float32),
        lax.psum(forget_trace.astype(jnp.bfloat16), "tp").astype(jnp.float32),
    )
    query_out = finish(
        query_weight,
        query_moment,
        query_rows,
        query_cols,
        query_col_root,
        results[0][0],
        query_outer,
        results[0][2],
        query_square,
    )
    forget_out = finish(
        forget_weight,
        forget_moment,
        forget_rows,
        forget_cols,
        forget_col_root,
        results[1][0],
        forget_outer,
        results[1][2],
        forget_square,
    )
    return (
        query_out[0],
        forget_out[0],
        query_out[1],
        forget_out[1],
        query_out[2],
        forget_out[2],
        query_out[3],
        forget_out[3],
        query_out[4],
        forget_out[4],
        query_out[5],
        forget_out[5],
    )


def linear_pairs(fs_size, tp_size, target):
    pairs = []
    for f in range(fs_size):
        for t in range(tp_size):
            to_f, to_t = target(f, t)
            pairs.append((f * tp_size + t, to_f * tp_size + to_t))
    return pairs


def gather_operands(keep, send, fs_size, tp_size):
    axes = ("fs", "tp")

    def move(value, target):
        return lax.ppermute(value, axes, linear_pairs(fs_size, tp_size, target))

    def partner(f, t):
        return (f, t ^ 1)

    def first_hop(f, t):
        return (f ^ 1, t) if t % 2 == 0 else (f, t ^ 2)

    def second_hop(f, t):
        return (f, t ^ 2) if t % 2 == 0 else (f ^ 1, t)

    lanes = [jnp.stack([keep, move(send, partner)])]
    for k in range(1, fs_size // 2):
        step = k & -k if k & (k - 1) == 0 else k & (k - 1) ^ k
        source = lanes[k ^ step]
        lanes.append(move(source, lambda f, t, step=step: (f ^ (2 * step), t)))
    sets = []
    nears = []
    for s, lane in enumerate(lanes):
        if s & 1:
            nears.append(move(nears[s ^ 1], lambda f, t: (f ^ 2, t)))
        else:
            nears.append(move(lane, first_hop))
        pair = jnp.stack([lane, nears[s]])
        far = move(pair, second_hop)
        sets.append((pair, far, move(pair, partner), move(far, partner)))
    return sets


def position():
    tp_at = lax.axis_index("tp")
    return tp_at & 1, tp_at >> 1, lax.axis_index("fs")


def assemble(place, pieces, x_set, y_set, sem):
    odd, upper = place[0], place[1]
    tokens, width = pieces[0].shape[2:]
    own = width // 2
    hidden = y_set.shape[1] // 2

    def copies(x_pieces, y_pieces):
        for p in range(2):
            rows = pl.ds(p * tokens, tokens)
            for h in range(2):
                for c in range(2):
                    col = pl.multiple_of(((upper ^ h) * 2 + c) * width, width)
                    pltpu.make_async_copy(
                        x_pieces[h].at[p, c], x_set.at[rows, pl.ds(col, width)], sem.at[0]
                    ).start()
                    for i in range(2):
                        pltpu.make_async_copy(
                            y_pieces[p].at[h, 1 - c, :, pl.ds(i * own, own)],
                            y_set.at[rows, pl.ds(i * hidden + (2 * h + c) * own, own)],
                            sem.at[1],
                        ).start()

    pair, far, pair_other, far_other = pieces

    @pl.when(odd == 0)
    def _():
        copies((pair, far), (pair_other, far_other))

    @pl.when(odd == 1)
    def _():
        copies((pair_other, far_other), (pair, far))


def assembled(x_set, y_set, sem):
    for k, whole in enumerate((x_set, y_set)):
        pltpu.make_async_copy(whole, whole, sem.at[k]).wait()


def product(x_set, y_set, cols):
    return lax.dot_general(
        x_set[...], y_set[:, cols], (((0,), (0,)), ((), ())), preferred_element_type=jnp.float32
    )


def sum_kernel(first, n_fetched, *refs):
    place = position()
    pieces, refs = refs[:4], refs[4:]
    if not first:
        refs = refs[1:]
    sources, refs = refs[:n_fetched], refs[n_fetched:]
    acc, fetched, (x_set, y_set, sem, fetch_sem) = refs[0], refs[1:-4], refs[-4:]
    assemble(place, pieces, x_set, y_set, sem)
    copies = [
        pltpu.make_async_copy(src, dst, fetch_sem.at[j])
        for j, (src, dst) in enumerate(zip(sources, fetched, strict=True))
    ]
    assembled(x_set, y_set, sem)
    for copy in copies:
        copy.start()
    total, chunk = acc.shape[1], x_set.shape[0]
    for at in range(0, total, chunk):
        cols = slice(at, at + chunk)
        part = product(x_set, y_set, cols)
        acc[:, cols] = part if first else acc[:, cols] + part
    for copy in copies:
        copy.wait()


def tail_kernel(*refs):
    place = position()
    pieces, acc, refs = refs[:4], refs[4], refs[5:]
    sides = [refs[6 * i : 6 * i + 6] for i in range(2)]
    refs = refs[12:]
    outs = [refs[6 * i : 6 * i + 6] for i in range(2)]
    refs = refs[12:]
    x_set, y_set, grad, roots, sem, store_sem = refs[:6]
    made = [refs[6 + 6 * i : 12 + 6 * i] for i in range(2)]
    odd, band = place[0], place[2]
    model, total = grad.shape
    hidden = total // 2
    own = pieces[0].shape[3] // 2
    rows_here = sides[0][0].shape[0]

    assemble(place, pieces, x_set, y_set, sem)
    roots[...] = jnp.zeros(roots.shape, roots.dtype)
    for i in range(2):
        for k in range(2):
            for h in range(own // HEAD):
                at = slice(h * HEAD, (h + 1) * HEAD)
                roots[i, k * own + h * HEAD : k * own + (h + 1) * HEAD, at] = sides[i][5][h]
    assembled(x_set, y_set, sem)

    chunk = x_set.shape[0]
    squares = [jnp.zeros((8, chunk), jnp.float32)] * 2
    for at in range(0, total, chunk):
        cols = slice(at, at + chunk)
        part = acc[:, cols] + product(x_set, y_set, cols)
        grad[:, cols] = part.astype(jnp.bfloat16)
        squares[at // hidden] += jnp.sum((part * part).reshape(-1, 8, chunk), axis=0)

    stores = []

    def store(src, dst, at):
        stores.append(pltpu.make_async_copy(src, dst, store_sem.at[at]))
        stores[-1].start()

    scales = []
    for i in range(2):
        _, row_root, weight, moment, cols, _ = sides[i]
        results, cols_next = made[i][:4], made[i][5]
        square = jnp.sum(squares[i], keepdims=True)
        scale = jnp.sqrt(model * hidden / (square + 1.0))
        scales.append(scale)
        mine = pl.multiple_of(i * hidden + odd * own, own)
        own_grad = grad[:, pl.ds(mine, own)]
        left = jnp.dot(row_root[...], own_grad, preferred_element_type=jnp.float32)
        left_high = left.astype(jnp.bfloat16)
        left_low = (left - left_high.astype(jnp.float32)).astype(jnp.bfloat16)
        column_total = lax.dot_general(
            own_grad, own_grad, (((0,), (0,)), ((), ())), preferred_element_type=jnp.float32
        )
        for h in range(own // HEAD):
            at = slice(h * HEAD, (h + 1) * HEAD)
            cols_next[h] = (
                stat_decay * cols[h]
                + (1.0 - stat_decay) / model * scale * scale * column_total[at, at]
            )
        precond = scale * jnp.dot(
            jnp.concatenate([left_high, left_low], axis=1),
            roots[i],
            preferred_element_type=jnp.float32,
        )
        moment_next = moment_decay * moment[...] + (1.0 - moment_decay) * precond
        update_step = moment_decay * moment_next + (1.0 - moment_decay) * precond
        master = weight[...] - learn_rate * update_step
        for to, value in zip(
            results, (master, master.astype(jnp.bfloat16), update_step, moment_next), strict=True
        ):
            to[...] = value
        for j, src in enumerate(results):
            store(src, outs[i][j], (i, j))
        store(cols_next, outs[i][5], (i, 4))
    first = pl.multiple_of(band * rows_here, rows_here)
    piece = 2 * own
    for i in range(2):
        rows, rows_next = sides[i][0], made[i][4]
        band_grad = grad[pl.ds(first, rows_here), i * hidden : (i + 1) * hidden]
        factor = (1.0 - stat_decay) / hidden * scales[i] * scales[i]
        for k in range(model // piece):
            at = slice(k * piece, (k + 1) * piece)
            part = lax.dot_general(
                band_grad,
                grad[at, i * hidden : (i + 1) * hidden],
                (((1,), (1,)), ((), ())),
                preferred_element_type=jnp.float32,
            )
            rows_next[:, at] = stat_decay * rows[:, at] + factor * part
            store(rows_next.at[:, at], outs[i][4].at[:, at], (i, 5 + k))
    for copy in stores:
        copy.wait()


def prepare_kernel(*refs):
    place = position()
    sources, (keep, send), held, sem = refs[:5], refs[5:7], refs[7:12], refs[12]
    copies = [
        pltpu.make_async_copy(src, dst, sem.at[j])
        for j, (src, dst) in enumerate(zip(sources, held, strict=True))
    ]
    for copy in copies:
        copy.start()
    for copy in copies:
        copy.wait()
    inputs, query_grad, forget_grad, forget_pre, lower_bound = held
    own = query_grad.shape[1]
    sigma_gate = jax.nn.sigmoid(forget_pre[...].astype(jnp.float32))
    forget_cot = (
        forget_grad[...].astype(jnp.float32)
        * (1.0 - lower_bound[...])
        * sigma_gate
        * (1.0 - sigma_gate)
    ).astype(jnp.bfloat16)

    def write(x_to, y_to):
        x_to[...] = inputs[...]
        y_to[:, :own] = query_grad[...]
        y_to[:, own:] = forget_cot

    @pl.when(place[0] == 0)
    def _():
        write(keep, send)

    @pl.when(place[0] == 1)
    def _():
        write(send, keep)


def gathered_plan(
    inputs,
    query_grad,
    forget_grad,
    forget_pre,
    lower_bound,
    query_weight,
    forget_weight,
    query_moment,
    forget_moment,
    query_rows,
    forget_rows,
    query_cols,
    forget_cols,
    query_row_root,
    forget_row_root,
    query_col_root,
    forget_col_root,
    fs_size,
    tp_size,
):
    vmem = pl.BlockSpec(memory_space=pltpu.VMEM)
    params = pltpu.CompilerParams(vmem_limit_bytes=21 * 2**20)
    hbm = pl.BlockSpec(memory_space=pltpu.HBM)
    saved = (inputs, query_grad, forget_grad, forget_pre, lower_bound[None])
    keep, send = pl.pallas_call(
        prepare_kernel,
        out_shape=(pltpu.VMEM(inputs.shape, inputs.dtype),) * 2,
        in_specs=[hbm] * 5,
        out_specs=[vmem] * 2,
        scratch_shapes=[pltpu.VMEM(v.shape, v.dtype) for v in saved]
        + [pltpu.SemaphoreType.DMA((5,))],
        compiler_params=params,
        name="prepare",
    )(*(pltpu.with_memory_space_constraint(v, pltpu.HBM) for v in saved))
    sets = gather_operands(keep, send, fs_size, tp_size)
    model = inputs.shape[1] * tp_size
    total = 2 * query_grad.shape[1] * tp_size
    sides = (
        (query_rows, query_row_root, query_weight, query_moment, query_cols, query_col_root),
        (forget_rows, forget_row_root, forget_weight, forget_moment, forget_cols, forget_col_root),
    )
    wide = jax.ShapeDtypeStruct(query_weight.shape, jnp.float32)
    narrow = jax.ShapeDtypeStruct(query_weight.shape, jnp.bfloat16)
    row_kind = jax.ShapeDtypeStruct(query_rows.shape, jnp.float32)
    col_kind = jax.ShapeDtypeStruct(query_cols.shape, jnp.float32)
    kinds = (wide, narrow, wide, wide, row_kind, col_kind)
    held = [pltpu.VMEM(k.shape, k.dtype) for k in kinds * 2]
    anywhere = pl.BlockSpec(memory_space=pl.ANY)
    set_scratch = [
        pltpu.VMEM((2 * inputs.shape[0], model), jnp.bfloat16),
        pltpu.VMEM((2 * inputs.shape[0], total), jnp.bfloat16),
    ]
    wanted = [[side[0] for side in sides], [v for side in sides for v in side[1:]]]
    wanted += [[]] * (len(sets) - 3)
    acc, fetched = [], []
    for s, pieces in enumerate(sets[:-1]):
        fetch = [pltpu.with_memory_space_constraint(v, pltpu.HBM) for v in wanted[s]]
        made = pl.pallas_call(
            partial(sum_kernel, not acc, len(fetch)),
            out_shape=[pltpu.VMEM((model, total), jnp.float32)]
            + [pltpu.VMEM(v.shape, v.dtype) for v in fetch],
            in_specs=[anywhere] * 4 + [vmem] * len(acc) + [hbm] * len(fetch),
            out_specs=[vmem] * (1 + len(fetch)),
            scratch_shapes=set_scratch
            + [pltpu.SemaphoreType.DMA((2,)), pltpu.SemaphoreType.DMA((max(len(fetch), 1),))],
            input_output_aliases={4: 0} if acc else {},
            compiler_params=pltpu.CompilerParams(vmem_limit_bytes=12 * 2**20),
        )(*pieces, *acc, *fetch)
        acc, fetched = made[:1], fetched + list(made[1:])
    half = len(fetched[2:]) // 2
    loaded = [fetched[0], *fetched[2 : 2 + half], fetched[1], *fetched[2 + half :]]
    operands = [*sets[-1], pltpu.with_memory_space_constraint(*acc, pltpu.VMEM)]
    operands += [pltpu.with_memory_space_constraint(v, pltpu.VMEM) for v in loaded]
    out = pl.pallas_call(
        tail_kernel,
        out_shape=kinds * 2,
        in_specs=[anywhere] * 4 + [vmem] * 13,
        out_specs=[hbm] * 12,
        scratch_shapes=set_scratch
        + [
            pltpu.VMEM((model, total), jnp.bfloat16),
            pltpu.VMEM((2, 2 * query_weight.shape[1], query_weight.shape[1]), jnp.bfloat16),
            pltpu.SemaphoreType.DMA((2,)),
            pltpu.SemaphoreType.DMA((2, 5 + model // query_weight.shape[1] // 2)),
        ]
        + held,
        compiler_params=params,
        name="tail",
    )(*operands)
    return tuple(v for both in zip(out[:6], out[6:], strict=True) for v in both)


def use_gathered(tokens, model, hidden, fs_size, tp_size):
    blocks = fs_size // 2
    square_grid = tp_size == 4 and fs_size % 2 == 0 and blocks & (blocks - 1) == 0
    return square_grid and tokens * (model + 2 * hidden) <= model * 2 * hidden


def on_device(fs_size, tp_size, inputs, query_grad, forget_grad, forget_pre, lower_bound, *rest):
    tokens = inputs.shape[0] * fs_size
    if use_gathered(tokens, inputs.shape[1] * tp_size, query_grad.shape[1] * tp_size, fs_size, tp_size):
        return gathered_plan(
            inputs, query_grad, forget_grad, forget_pre, lower_bound, *rest, fs_size, tp_size
        )
    sigma_gate = jax.nn.sigmoid(forget_pre.astype(jnp.float32))
    forget_cot = (
        forget_grad.astype(jnp.float32) * (1.0 - lower_bound) * sigma_gate * (1.0 - sigma_gate)
    ).astype(jnp.bfloat16)
    return summed_plan(inputs, query_grad, forget_cot, *rest)


def solution(mesh):
    in_specs = (
        P("fs", "tp"),
        P("fs", "tp"),
        P("fs", "tp"),
        P("fs", "tp"),
        P("tp"),
        P("fs", "tp"),
        P("fs", "tp"),
        P("fs", "tp"),
        P("fs", "tp"),
        P("fs", None),
        P("fs", None),
        P("tp", None, None),
        P("tp", None, None),
        P("fs", None),
        P("fs", None),
        P("tp", None, None),
        P("tp", None, None),
    )
    out_specs = (
        P("fs", "tp"),
        P("fs", "tp"),
        P("fs", "tp"),
        P("fs", "tp"),
        P("fs", "tp"),
        P("fs", "tp"),
        P("fs", "tp"),
        P("fs", "tp"),
        P("fs", None),
        P("fs", None),
        P("tp", None, None),
        P("tp", None, None),
    )
    sizes = (mesh.shape["fs"], mesh.shape["tp"])
    return jax.shard_map(
        partial(on_device, *sizes), mesh=mesh, in_specs=in_specs, out_specs=out_specs, check_vma=False
    )
```
